256 devices in a mesh: grp: 2 (over z), st: 16 (over y, core), tp: 8 (over x).
Axes of the slice: x: 8, y: 8, z: 2, core: 2. Of those that a mesh axis runs over, the one named last changes fastest.
The devices are a block of a 8x8x16 slice.
Arguments:
- tokens: bfloat16 [16384, 2048], P(('grp', 'st')), parts along dimension 0, may hold values from -6 to 6, as said below
- store: bfloat16 [256, 128, 2048], P(('grp', 'st')), parts along dimension 0, may hold values from -6 to 6, as said below
- passage_ids: int32 [256, 4], P(('grp', 'st')), parts along dimension 0, may hold values from 0 to 127, as said below
- mix_gain: float32 [2048], replicated, may hold values from 0.1 to 1.9
- glu_value: bfloat16 [2048, 1024], P(None, 'tp'), may hold values from -0.125 to 0.125
- glu_gate: bfloat16 [2048, 1024], P(None, 'tp'), may hold values from -0.125 to 0.125
- conv_taps: bfloat16 [31, 1024], P(None, 'tp'), may hold values from -5 to 5
- channel_gain: float32 [1024], P('tp'), may hold values from 0.1 to 1.9
- mix_out: bfloat16 [1024, 2048], P('tp'), may hold values from -0.1875 to 0.1875
- query_gain: float32 [2048], replicated, may hold values from 0.1 to 1.9
- passage_gain: float32 [2048], replicated, may hold values from 0.1 to 1.9
- query_proj: bfloat16 [2048, 2048], P(None, 'tp'), may hold values from -1 to 1
- key_proj: bfloat16 [2048, 2048], P(None, 'tp'), may hold values from -1 to 1
- value_proj: bfloat16 [2048, 2048], P(None, 'tp'), may hold values from -0.125 to 0.125
- attn_out: bfloat16 [2048, 2048], P('tp'), may hold values from -0.125 to 0.125
- blend_gain: float32 [2048], replicated, may hold values from 0.5 to 3
Outputs:
- blended: bfloat16 [16384, 2048], P(('grp', 'st', 'tp')), parts along dimension 0
The draws below stay inside these ranges and needn't reach their ends.
There are 2 independent parts, one for each index of `grp`. The reference program is written for one: setup_inputs(seed, part) draws one part's arguments, and reference() takes and returns one part's arrays. A program takes and returns all parts, laid end to end along the dimension named above; an argument that names none is the same for every part. Nothing has to cross between parts.
Inputs may be any that keep to these rules, and one draw needn't show every extreme that they name: `tokens`: standard normal entries clipped to the range. `store`: standard normal entries clipped to the range. `passage_ids`: passage p is held by index p // 8 of st. The 32 requests of the 8 blocks of one index of st (repeats counted) name at most 4 passages held by any one index of st, and in every draw one index of st receives exactly 4 requests from every index of st.
All inputs are finite; a program needn't handle non-finite values.
Results may differ from the reference program's by a relative error of at most 0.01575.
The reference program's roundings to bfloat16 on the way count: a program that leaves them out, or rounds other values in their place, can miss the bound.
Values may be sent and summed in bfloat16 or wider, within the bound.
A program may use at most 128 MiB of HBM per device.

```python
import jax
import jax.numpy as jnp
from jax import lax

D = 2048
CA = 1024
HEADS = 8
KW = 31
SEQ_LEN = 128
BLK = 64
NP = 4
PROWS = 128
PASS_DEV = 8
TOKENS = 8192
NB_DEV = 8
BLOCKS = 128
RQ = 32
MOST = 4
PASSAGES = 128
N_ST = 16
N_TP = 8


def request_table(key):
    hot_owner = jax.random.randint(jax.random.fold_in(key, 1), (), 0, N_ST)
    positions = jnp.arange(RQ)

    def one_device(device, dev_key):
        first_turn = (device - 1 - hot_owner) % N_ST - 1
        spread_turn = (first_turn + positions - MOST) % (N_ST - 1)
        owners_of = jnp.where(positions < MOST, hot_owner, (hot_owner + 1 + spread_turn) % N_ST)
        owners_of = owners_of[jax.random.permutation(dev_key, RQ)]
        local_index = jax.random.randint(jax.random.fold_in(dev_key, 3), (RQ,), 0, PASS_DEV)
        return (owners_of * PASS_DEV + local_index).reshape(NB_DEV, NP)
    dev_keys = jax.random.split(jax.random.fold_in(key, 2), N_ST)
    table = jax.vmap(one_device)(jnp.arange(N_ST), dev_keys)
    return table.reshape(BLOCKS, NP).astype(jnp.int32)


def store_rows(key):
    return jnp.clip(jax.random.normal(jax.random.fold_in(key, 12), (PASSAGES, PROWS, D), jnp.float32), -6.0, 6.0)


def draw_passage_ids(key, part):
    return request_table(jax.random.fold_in(key, 11))


def draw_store(key, part):
    return store_rows(key).astype(jnp.bfloat16)


def draw_tokens(key, part):
    plain_rows = jnp.clip(jax.random.normal(jax.random.fold_in(key, 13), (TOKENS, D), jnp.float32), -6.0, 6.0)
    return plain_rows.astype(jnp.bfloat16)


def draw_conv_taps(key, part):
    channel = jnp.arange(CA).astype(jnp.float32)
    channel_scale = jnp.exp(1.5 * (2.0 * channel / CA - 1.0)) * KW ** (-0.5)
    tap_draw = jnp.clip(jax.random.normal(jax.random.fold_in(key, 31), (KW, CA), jnp.float32), -6.0, 6.0)
    return jnp.clip(tap_draw * channel_scale, -5.0, 5.0).astype(jnp.bfloat16)


def draw_query_proj(key, part):
    fresh_draw = jax.random.normal(jax.random.fold_in(key, 22), (D, D), jnp.float32) * D ** (-0.5)
    return jnp.clip(fresh_draw, -1.0, 1.0).astype(jnp.bfloat16)


def draw_key_proj(key, part):
    fresh_draw = jax.random.normal(jax.random.fold_in(key, 23), (D, D), jnp.float32) * D ** (-0.5)
    return jnp.clip(fresh_draw, -1.0, 1.0).astype(jnp.bfloat16)


def shard_levels(stream_key, dims, pieces, smallest, high):
    gain, own = 1.0, jax.random.fold_in(stream_key, 6)
    for axis_at, blocks in pieces:
        steps = jnp.exp(jax.random.uniform(jax.random.fold_in(own, axis_at), (blocks,), jnp.float32, smallest / len(pieces), high / len(pieces)))
        gain = gain * jnp.repeat(steps, dims[axis_at] // blocks).reshape([-1 if axis == axis_at else 1 for axis in range(len(dims))])
    return gain


def normal_values(own_key, dims, scale, reach, cuts=(), dtype=jnp.bfloat16):
    drawn = jax.random.normal(own_key, dims, jnp.float32) * scale
    if len(cuts) > 0:
        drawn = shard_levels(own_key, dims, cuts, -0.22, 0.18) * drawn
    return jnp.clip(drawn, min=-reach, max=reach).astype(dtype)


def setup_inputs(seed: int = 0, part: int = 0) -> dict:
    streams_of = jax.random.split(jax.random.key(seed), 17)
    part_keys = jax.random.split(jax.random.fold_in(streams_of[16], part), 17)
    return {
        "tokens": draw_tokens(jax.random.fold_in(jax.random.fold_in(streams_of[16], part), 71), part),
        "store": draw_store(jax.random.fold_in(jax.random.fold_in(streams_of[16], part), 71), part),
        "passage_ids": draw_passage_ids(jax.random.fold_in(jax.random.fold_in(streams_of[16], part), 71), part),
        "mix_gain": jnp.clip(1.0 + 0.18 * jax.random.normal(streams_of[3], (D,), jnp.float32), 0.1, 1.9),
        "glu_value": normal_values(streams_of[4], (D, CA), D ** -0.5, 0.125, ((1, 8),)),
        "glu_gate": normal_values(streams_of[5], (D, CA), D ** -0.5, 0.125, ((1, 8),)),
        "conv_taps": draw_conv_taps(jax.random.fold_in(streams_of[16], 71), part),
        "channel_gain": jnp.clip(1.0 + 0.18 * jax.random.normal(streams_of[7], (CA,), jnp.float32), 0.1, 1.9),
        "mix_out": normal_values(streams_of[8], (CA, D), CA ** -0.5, 0.1875, ((0, 8),)),
        "query_gain": jnp.clip(1.0 + 0.18 * jax.random.normal(streams_of[9], (D,), jnp.float32), 0.1, 1.9),
        "passage_gain": jnp.clip(1.0 + 0.18 * jax.random.normal(streams_of[10], (D,), jnp.float32), 0.1, 1.9),
        "query_proj": draw_query_proj(jax.random.fold_in(streams_of[16], 71), part),
        "key_proj": draw_key_proj(jax.random.fold_in(streams_of[16], 71), part),
        "value_proj": normal_values(streams_of[13], (D, D), D ** -0.5, 0.125, ((1, 8),)),
        "attn_out": normal_values(streams_of[14], (D, D), D ** -0.5, 0.125, ((0, 8),)),
        "blend_gain": jnp.clip(jax.random.uniform(streams_of[15], (D,), jnp.float32, 0.5, 3.0), 0.5, 3.0),
    }


EPS = 1e-06

def rms_rows(row_data, gain_vec):
    floats = row_data.astype(jnp.float32)
    inv_scale = lax.rsqrt(lax.optimization_barrier(jnp.mean(floats * floats, axis=-1, keepdims=True)) + EPS)
    return (floats * inv_scale * gain_vec.astype(jnp.float32)).astype(jnp.bfloat16)

def depthwise(gated_rows, conv_taps):
    span_width = conv_taps.shape[0]
    half_span = (span_width - 1) // 2
    seq_length = gated_rows.shape[1]
    padded = jnp.pad(gated_rows.astype(jnp.float32), ((0, 0), (half_span, span_width - 1 - half_span), (0, 0)))
    running = jnp.zeros(gated_rows.shape, jnp.float32)
    for tap_index in range(span_width):
        running = running + padded[:, tap_index:tap_index + seq_length] * conv_taps[tap_index].astype(jnp.float32)
    return running

def passage_attention(queries, keys_values, head_count):
    groups, block_len, span_width = queries.shape
    head_dim = span_width // head_count
    row_count = keys_values.shape[1]
    query_heads = queries.astype(jnp.float32).reshape(groups, block_len, head_count, head_dim)
    key_heads = keys_values[:, :, :span_width].astype(jnp.float32).reshape(groups, row_count, head_count, head_dim)
    value_heads = keys_values[:, :, span_width:].astype(jnp.float32).reshape(groups, row_count, head_count, head_dim)
    scores = jnp.einsum('gqhd,grhd->ghqr', query_heads, key_heads) * head_dim ** (-0.5)
    row_top = lax.optimization_barrier(jnp.max(scores, axis=-1))
    exponent = jnp.exp(scores - row_top[..., None])
    row_sum = lax.optimization_barrier(jnp.sum(exponent, axis=-1))
    weights = exponent.astype(jnp.bfloat16).astype(jnp.float32)
    outputs = jnp.einsum('ghqr,grhd->gqhd', weights, value_heads).astype(jnp.bfloat16)
    return (outputs.reshape(groups, block_len, span_width), row_top, row_sum)

def combine(outs, tops, sums, head_count):
    batch_count, passage_count, block_len, span_width = outs.shape
    head_dim = span_width // head_count
    best_top = lax.optimization_barrier(jnp.max(tops, axis=1, keepdims=True))
    weight = jnp.exp(tops - best_top)
    numerator = jnp.einsum('bphq,bpqhd->bqhd', weight, outs.astype(jnp.float32).reshape(batch_count, passage_count, block_len, head_count, head_dim))
    denominator = lax.optimization_barrier(jnp.sum(weight * sums, axis=1))
    result = numerator / jnp.transpose(denominator, (0, 2, 1))[..., None]
    return result.reshape(batch_count, block_len, span_width).astype(jnp.bfloat16)

def reference(tokens, store, passage_ids, mix_gain, glu_value, glu_gate, conv_taps, channel_gain, mix_out, query_gain, passage_gain, query_proj, key_proj, value_proj, attn_out, blend_gain):
    mix_input = rms_rows(tokens, mix_gain)
    value_part = jnp.dot(mix_input, glu_value, preferred_element_type=jnp.float32)
    gate_part = jnp.dot(mix_input, glu_gate, preferred_element_type=jnp.float32)
    gated_rows = (value_part * jax.nn.sigmoid(gate_part)).astype(jnp.bfloat16)
    conv_rows = depthwise(gated_rows.reshape(-1, SEQ_LEN, CA), conv_taps).reshape(-1, CA)
    row_mean = lax.optimization_barrier(jnp.mean(conv_rows, axis=1, keepdims=True))
    row_var = lax.optimization_barrier(jnp.mean(conv_rows * conv_rows, axis=1, keepdims=True)) - row_mean * row_mean
    activation = jax.nn.silu((conv_rows - row_mean) * lax.rsqrt(row_var + EPS) * channel_gain.astype(jnp.float32)).astype(jnp.bfloat16)
    queries = jnp.dot(rms_rows(tokens, query_gain), query_proj, preferred_element_type=jnp.float32).astype(jnp.bfloat16)
    passage_rows = rms_rows(store.reshape(-1, D), passage_gain)
    key_rows = jnp.dot(passage_rows, key_proj, preferred_element_type=jnp.float32).astype(jnp.bfloat16)
    value_rows = jnp.dot(passage_rows, value_proj, preferred_element_type=jnp.float32).astype(jnp.bfloat16)
    memory = jnp.concatenate([key_rows, value_rows], axis=1).reshape(store.shape[0], store.shape[1], 2 * D)

    def one_block(inputs):
        block_queries, block_ids = inputs
        wanted = memory[block_ids]
        repeated = jnp.broadcast_to(block_queries[None], (NP, BLK, D))
        part_out, part_top, part_sum = passage_attention(repeated, wanted, HEADS)
        return combine(part_out[None], part_top[None], part_sum[None], HEADS)[0]
    attended = lax.map(one_block, (queries.reshape(-1, BLK, D), passage_ids)).reshape(-1, D)
    channel_group = CA // N_TP
    column_group = D // N_TP
    running = jnp.zeros((tokens.shape[0], D), jnp.float32)
    for shard_index in range(N_TP):
        conv_part = jnp.dot(activation[:, shard_index * channel_group:(shard_index + 1) * channel_group], mix_out[shard_index * channel_group:(shard_index + 1) * channel_group], preferred_element_type=jnp.float32)
        attn_part = jnp.dot(attended[:, shard_index * column_group:(shard_index + 1) * column_group], attn_out[shard_index * column_group:(shard_index + 1) * column_group], preferred_element_type=jnp.float32)
        partial_value = (conv_part + blend_gain.astype(jnp.float32) * attn_part).astype(jnp.bfloat16)
        partial_value = lax.optimization_barrier(partial_value)
        running = running + partial_value.astype(jnp.float32)
    return running.astype(jnp.bfloat16)
```

```python
import functools

import jax
import jax.numpy as jnp
from jax import lax
from jax.experimental import pallas as pl
from jax.experimental.pallas import tpu as pltpu
from jax.sharding import PartitionSpec as P

CA = 1024
HD = 256
SEQ_LEN = 128
CORES = 2
LANES = 128
EPS = 1e-06
EMPTY = -1e30
MESH = pl.DeviceIdType.MESH
F32 = jnp.float32
BF16 = jnp.bfloat16


def remote(src, dst, send_sem, recv_sem, **target):
    return pltpu.make_async_remote_copy(
        src_ref=src, dst_ref=dst, send_sem=send_sem, recv_sem=recv_sem,
        device_id=target, device_id_type=MESH,
    )


def place_of(distance, n):
    half = n // 2
    return jnp.where(distance >= half, 2 * (distance - half), 2 * (half - distance) - 1)


def order_of(n):
    half = n // 2
    order = [half]
    for j in range(1, half):
        order += [half - j, half + j]
    return order + [0]


def normed_rows(dst, src, gain, rows, step=16):
    @pl.loop(0, rows // step)
    def _(i):
        at = pl.ds(pl.multiple_of(i * step, step), step)
        x = src[at, :].astype(F32)
        inv = lax.rsqrt(jnp.mean(x * x, axis=-1, keepdims=True) + EPS)
        dst[at, :] = (x * inv * gain[...]).astype(BF16)


def serve_kernel(
    n_st, n_tp, slots, blocks, per_block,
    tok_hbm, store_hbm, wq_hbm, wk_hbm, wv_hbm, qgain, pgain, table,
    acc, stats,
    tok, store, wq, wk, wv, xn, *rest,
):
    ring = n_st // CORES
    qall = rest[:ring]
    kall, vall, outs, ml, tabv, tabs, load_sem, q_send, q_recv, kv_send, kv_recv, t_send, t_recv, s_sem = rest[ring:]
    me = lax.axis_index("st")
    x_me = lax.axis_index("tp")
    core = lax.rem(me, CORES)
    y_me = me // CORES
    partner = me + 1 - 2 * core

    def chip(d):
        return lax.rem(me + CORES * d, n_st)

    right, left = chip(1), chip(ring - 1)
    groups = tok_hbm.shape[0] // 128
    passages = store_hbm.shape[0]
    half = ring // 2
    per_group = blocks // groups

    loads = []

    def load(src, dst):
        copy = pltpu.make_async_copy(src, dst, load_sem.at[len(loads)])
        copy.start()
        loads.append(copy)
        return copy

    wq_load = load(wq_hbm, wq)
    tok_loads = [load(tok_hbm.at[pl.ds(g * 128, 128)], tok.at[pl.ds(g * 128, 128)]) for g in range(groups)]
    wk_load = load(wk_hbm, wk)
    wv_load = load(wv_hbm, wv)
    store_loads = [load(store_hbm.at[p], store.at[p]) for p in range(passages)]

    barrier = pltpu.get_barrier_semaphore()
    for d in range(1, ring):
        pl.semaphore_signal(barrier, inc=1, device_id={"st": chip(d)}, device_id_type=MESH)
    pl.semaphore_signal(barrier, inc=1, device_id={"st": partner}, device_id_type=MESH)

    outs[slots] = jnp.zeros(outs.shape[1:], outs.dtype)
    ml[slots, 0:1] = jnp.full((1, LANES), EMPTY, F32)
    ml[slots, 1:2] = jnp.zeros((1, LANES), F32)

    sends = []

    def send(copy):
        copy.start()
        sends.append(copy)

    def part(rel, g):
        return qall[rel].at[pl.ds(per_group * g, per_group)]

    tok_loads[0].wait()
    normed_rows(xn, tok.at[pl.ds(0, 128)], qgain, 128)
    wq_load.wait()
    for g in range(groups):
        if g > 0:
            tok_loads[g].wait()
            normed_rows(xn, tok.at[pl.ds(g * 128, 128)], qgain, 128)
        q = jnp.dot(xn[...], wq[...], preferred_element_type=F32).astype(BF16)
        for i in range(per_group):
            qall[0][per_group * g + i] = q[i * (128 // per_group) : (i + 1) * (128 // per_group)]
        if g == 0:
            pl.semaphore_wait(barrier, ring)
            for d in range(1, ring):
                send(remote(table.at[lax.rem(y_me + d, ring)], tabv.at[ring - d], t_send.at[d - 1],
                            t_recv.at[ring - d - 1], st=chip(d)))
        send(remote(part(0, g), part(ring - 1, g), q_send.at[0, g], q_recv.at[0, g], st=right))
        send(remote(part(0, g), part(1, g), q_send.at[1, g], q_recv.at[1, g], st=left))

    own_table = pltpu.make_async_copy(table.at[y_me], tabv.at[0], s_sem.at[1])
    own_table.start()

    def event(e):
        last = (half - 1) * groups
        if e < last:
            hop, g = e // groups + 1, e % groups
            for side in range(2):
                rel = ring - hop if side == 0 else hop
                here = part(rel, g)
                remote(here, here, q_send.at[side, e], q_recv.at[side, e], st=right).wait_recv()
                if hop < half - 1:
                    nxt = e + groups
                elif side == 0 and g < groups // 2:
                    nxt = last + g
                elif side == 1 and g >= groups // 2:
                    nxt = last + g - groups // 2
                else:
                    continue
                there = part(rel - 1 if side == 0 else rel + 1, g)
                send(remote(here, there, q_send.at[side, nxt], q_recv.at[side, nxt],
                            st=right if side == 0 else left))
        else:
            for side in range(2):
                here = part(half, e - last + side * (groups // 2))
                remote(here, here, q_send.at[side, 0], q_recv.at[side, e], st=right).wait_recv()

    def keys_values(p):
        store_loads[p].wait()
        normed_rows(xn, store.at[p], pgain, 128)
        if p == 0:
            wk_load.wait()
            wv_load.wait()
        at = core * passages + p
        kall[at] = jnp.dot(xn[...], wk[...], preferred_element_type=F32).astype(BF16)
        v = jnp.dot(xn[...], wv[...], preferred_element_type=F32)
        vall[at] = jnp.concatenate([v[:, :LANES].T, v[:, LANES:].T], axis=1).astype(BF16)
        send(remote(kall.at[at], kall.at[at], kv_send.at[0, p], kv_recv.at[0, p], st=partner))
        send(remote(vall.at[at], vall.at[at], kv_send.at[1, p], kv_recv.at[1, p], st=partner))

    low_half = lax.broadcasted_iota(jnp.int32, (LANES, LANES), 1) < LANES // 2

    def attend(rel):
        for k in range(slots):
            q = qall[rel][tabs[rel, 0, k]]
            p = tabs[rel, 0, slots + k]
            s = lax.dot_general(
                kall[p], jnp.concatenate([q, q], axis=0), (((1,), (1,)), ((), ())), preferred_element_type=F32
            ) * HD ** (-0.5)
            top = jnp.max(s, axis=0, keepdims=True)
            e = jnp.exp(s - top)
            ml[k, 0:1] = top
            ml[k, 1:2] = jnp.sum(e, axis=0, keepdims=True)
            w = jnp.concatenate([jnp.where(low_half, e, 0.0), jnp.where(low_half, 0.0, e)], axis=0).astype(BF16)
            outs[k] = jnp.dot(vall[p], w, preferred_element_type=F32).astype(BF16)

        @pl.loop(0, blocks)
        def _(distance):
            b = lax.rem(x_me + distance, blocks)
            at = [tabs[rel, 0, 2 * slots + b * per_block + j] for j in range(per_block)]
            mls = [ml[i] for i in at]
            best = functools.reduce(jnp.maximum, [a[0:1] for a in mls])
            scale = [jnp.exp(a[0:1] - best) for a in mls]
            total = sum(f * a[1:2] for f, a in zip(scale, mls))
            num = sum(f * outs[i].astype(F32) for f, i in zip(scale, at))
            place = place_of(distance, n_tp)
            acc[rel, place] = num.astype(BF16)
            stats[rel, place, 0:1] = best
            stats[rel, place, 1:2] = total

    def all_here():
        for p in range(passages):
            other = (1 - core) * passages + p
            for i, ref in enumerate((kall, vall)):
                remote(ref.at[other], ref.at[other], kv_send.at[i, p], kv_recv.at[i, p], st=partner).wait_recv()
        own_table.wait()
        for d in range(1, ring):
            here = tabv.at[d]
            remote(here, here, t_send.at[d - 1], t_recv.at[d - 1], st=partner).wait_recv()
        to_scalar = pltpu.make_async_copy(tabv, tabs, s_sem.at[0])
        to_scalar.start()
        to_scalar.wait()

    events = (half - 1) * groups + groups // 2
    done = 0
    for p in range(passages):
        keys_values(p)
        if p >= 1:
            event(done)
            done += 1
    all_here()
    turns = [0]
    for hop in range(1, half):
        turns += [ring - hop, hop]
    turns += [half]
    for rel in turns:
        hop = min(rel, ring - rel)
        need = min(hop * groups, events) if hop < half else events
        while done < need:
            event(done)
            done += 1
        attend(rel)
        if done < events:
            event(done)
            done += 1
    for copy in sends:
        copy.wait_send()


def serve(tokens, store, query_proj, key_proj, value_proj, query_gain, passage_gain, table, slots, blocks, per_block):
    n_st, n_tp = lax.axis_size("st"), lax.axis_size("tp")
    ring = n_st // CORES
    rows, width = tokens.shape
    passages, prows, _ = store.shape
    groups = rows // 128
    block_len = rows // blocks
    assert prows == 128 and query_proj.shape[1] == HD and block_len * 2 == LANES and blocks == n_tp
    events = (ring // 2 - 1) * groups + groups // 2
    hbm = pl.BlockSpec(memory_space=pl.ANY)
    vmem = pl.BlockSpec(memory_space=pltpu.VMEM)
    return pl.pallas_call(
        functools.partial(serve_kernel, n_st, n_tp, slots, blocks, per_block),
        out_shape=(
            jax.ShapeDtypeStruct((ring, blocks, LANES, LANES), BF16),
            jax.ShapeDtypeStruct((ring, blocks, 2, LANES), F32),
        ),
        in_specs=[hbm] * 5 + [vmem] * 3,
        out_specs=(vmem, vmem),
        scratch_shapes=[
            pltpu.VMEM((rows, width), BF16),
            pltpu.VMEM(store.shape, BF16),
            pltpu.VMEM(query_proj.shape, BF16),
            pltpu.VMEM(key_proj.shape, BF16),
            pltpu.VMEM(value_proj.shape, BF16),
            pltpu.VMEM((128, width), BF16),
            *[pltpu.VMEM((blocks, block_len, HD), BF16) for _ in range(ring)],
            pltpu.VMEM((CORES * passages, prows, HD), BF16),
            pltpu.VMEM((CORES * passages, LANES, 2 * prows), BF16),
            pltpu.VMEM((slots + 1, LANES, LANES), BF16),
            pltpu.VMEM((slots + 1, 2, LANES), F32),
            pltpu.VMEM(table.shape, jnp.int32),
            pltpu.SMEM(table.shape, jnp.int32),
            pltpu.SemaphoreType.DMA((3 + groups + passages,)),
            pltpu.SemaphoreType.DMA((2, events)),
            pltpu.SemaphoreType.DMA((2, events)),
            pltpu.SemaphoreType.DMA((2, passages)),
            pltpu.SemaphoreType.DMA((2, passages)),
            pltpu.SemaphoreType.DMA((ring - 1,)),
            pltpu.SemaphoreType.DMA((ring - 1,)),
            pltpu.SemaphoreType.DMA((2,)),
        ],
        compiler_params=pltpu.CompilerParams(
            collective_id=0, has_side_effects=True, vmem_limit_bytes=50 * 2**20
        ),
        name="serve",
    )(tokens, store, query_proj, key_proj, value_proj, query_gain, passage_gain, table)


def merged(a, b):
    best = jnp.maximum(a[1], b[1])
    fa, fb = jnp.exp(a[1] - best), jnp.exp(b[1] - best)
    return fa * a[0] + fb * b[0], best, fa * a[2] + fb * b[2]


def blend_kernel(
    n_st, n_tp,
    acc, stats, conv, sums, cgain, mix, attn, blend,
    out,
    ycw, yccw, scw, sccw, xa, xcw, xccw, act, allsums,
    y_send, y_recv, x_send, x_recv, c_send, c_recv,
):
    me = lax.axis_index("st")
    x_me = lax.axis_index("tp")
    ring = n_st // CORES
    half = ring // 2
    xhalf = n_tp // 2
    right, left = lax.rem(me + CORES, n_st), lax.rem(me + n_st - CORES, n_st)
    east, west = lax.rem(x_me + 1, n_tp), lax.rem(x_me + n_tp - 1, n_tp)
    blocks, block_len, width = xa.shape[0] * n_tp, xa.shape[1], xa.shape[2]
    wide = width // 2

    barrier = pltpu.get_barrier_semaphore()
    for who in (right, left):
        pl.semaphore_signal(barrier, inc=1, device_id={"st": who}, device_id_type=MESH)
    for d in range(1, n_tp):
        pl.semaphore_signal(barrier, inc=1, device_id={"tp": lax.rem(x_me + d, n_tp)}, device_id_type=MESH)
    pl.semaphore_wait(barrier, n_tp + 1)

    sends = []

    def send(copy):
        copy.start()
        sends.append(copy)

    for d in range(1, n_tp):
        send(remote(sums, allsums.at[n_tp - d], c_send.at[d - 1], c_recv.at[n_tp - d - 1],
                    tp=lax.rem(x_me + d, n_tp)))

    places = order_of(n_tp)
    chunks = [[0]] + [[2 * j - 1, 2 * j] for j in range(1, xhalf)] + [[n_tp - 1]]
    start_cw = {}
    for c, chunk in enumerate(chunks):
        for i, p in enumerate(chunk):
            start_cw[p] = half if (i == 0 and c < len(chunks) - 1) else half - 1

    sides = (
        (ycw, scw, right, lambda d: d),
        (yccw, sccw, left, lambda d: ring - d),
    )

    def start_of(side, p):
        return start_cw[p] if side == 0 else 2 * half - 1 - start_cw[p]

    def y_send_out(side, p, d, num, stat):
        data, st_, who, _ = sides[side]
        send(remote(num, data.at[p, d - 1], y_send.at[side, p, d - 1, 0], y_recv.at[side, p, d - 1, 0], st=who))
        send(remote(stat, st_.at[p, d - 1], y_send.at[side, p, d - 1, 1], y_recv.at[side, p, d - 1, 1], st=who))

    def y_arrived(side, p, d):
        data, st_, _, _ = sides[side]
        for i, ref in enumerate((data.at[p, d], st_.at[p, d])):
            remote(ref, ref, y_send.at[side, p, d, i], y_recv.at[side, p, d, i], st=right).wait_recv()
        return data[p, d].astype(F32), st_[p, d, 0:1], st_[p, d, 1:2]

    def own(rel, p):
        return acc[rel, p].astype(F32), stats[rel, p, 0:1], stats[rel, p, 1:2]

    def y_start(c, u):
        for p in chunks[c]:
            for side in range(2):
                d = start_of(side, p)
                if d == half - u:
                    rel = sides[side][3](d)
                    y_send_out(side, p, d, acc.at[rel, p], stats.at[rel, p])

    def y_stage(c, u):
        d = half - u
        for p in chunks[c]:
            for side in range(2):
                if d < start_of(side, p):
                    data, st_, _, rel = sides[side]
                    num, best, total = merged(y_arrived(side, p, d), own(rel(d), p))
                    data[p, d] = num.astype(BF16)
                    st_[p, d, 0:1] = best
                    st_[p, d, 1:2] = total
                    y_send_out(side, p, d, data.at[p, d], st_.at[p, d])

    def y_home(p):
        num, best, total = merged(merged(y_arrived(0, p, 0), own(0, p)), y_arrived(1, p, 0))
        t = (num / total).T.astype(BF16)
        return jnp.concatenate([t[:block_len], t[block_len:]], axis=1)

    def activations():
        for d in range(1, n_tp):
            here = allsums.at[d]
            remote(here, here, c_send.at[d - 1], c_recv.at[d - 1], tp=east).wait_recv()
        total = sums[...]
        for d in range(1, n_tp):
            total = total + allsums[d]
        groups = total.shape[0] // 2
        mean = total[:groups] / CA
        var = total[groups:] / CA - mean * mean
        cols = jnp.concatenate([mean, lax.rsqrt(var + EPS)], axis=0).T
        per = 128 // block_len
        for g in range(groups):
            z = conv[pl.ds(g * 128, 128), :]
            z = (z - cols[:, g : g + 1]) * cols[:, groups + g : groups + g + 1] * cgain[...]
            z = (z / (1.0 + jnp.exp(-z))).astype(BF16)
            for i in range(per):
                act[g * per + i] = z[i * block_len : (i + 1) * block_len]

    def x_wait(side, k, h):
        data = (xcw, xccw)[side]
        here = data.at[k, :, pl.ds(h * wide, wide)]
        remote(here, here, x_send.at[side, k, h], x_recv.at[side, k, h], tp=east).wait_recv()

    def x_out(side, k, h, src):
        data = (xcw, xccw)[side]
        send(remote(src, data.at[k - 1, :, pl.ds(h * wide, wide)], x_send.at[side, k - 1, h],
                    x_recv.at[side, k - 1, h], tp=east if side == 0 else west))

    tile = 512

    def project(c):
        chunk = chunks[c]
        k = xhalf - c
        rows_a = jnp.concatenate([y_home(p) for p in chunk], axis=0)
        rows_p = jnp.concatenate([act[lax.rem(x_me + places[p], n_tp)] for p in chunk], axis=0)
        for t in range(width // tile):
            at = pl.ds(t * tile, tile)
            h = t * tile // wide
            first, last = t * tile % wide == 0, (t + 1) * tile % wide == 0
            y = jnp.dot(rows_p, mix[:, at], preferred_element_type=F32) + blend[:, at] * jnp.dot(
                rows_a, attn[:, at], preferred_element_type=F32
            )
            if k == xhalf:
                xa[0, :, at] = y.astype(BF16)
                if last:
                    x_out(h, k, h, xa.at[0, :, pl.ds(h * wide, wide)])
            elif k > 0:
                for side in range(2):
                    data = (xcw, xccw)[side]
                    mine = y[side * block_len : (side + 1) * block_len]
                    if k < xhalf - 1 or h == side:
                        if first:
                            x_wait(side, k, h)
                        mine = mine + data[k, :, at].astype(F32)
                    data[k, :, at] = mine.astype(BF16)
                    if last:
                        x_out(side, k, h, data.at[k, :, pl.ds(h * wide, wide)])
            else:
                for side in range(2):
                    if first:
                        x_wait(side, 0, h)
                y = y + xcw[0, :, at].astype(F32) + xccw[0, :, at].astype(F32)
                out[:, at] = y.astype(BF16)

    n_chunks = len(chunks)
    for turn in range(n_chunks + half):
        for c in range(n_chunks):
            u = turn - c
            if 1 <= u < half:
                y_stage(c, u)
        for c in range(n_chunks):
            if turn == max(c - 1, 0):
                y_start(c, 0)
            if turn == c + 1 - (1 if c > 1 else 0):
                y_start(c, 1)
        if turn == 1:
            activations()
        c = turn - half
        if 0 <= c < n_chunks:
            project(c)
    for copy in sends:
        copy.wait_send()


def blended_rows(acc, stats, conv, sums, channel_gain, mix_out, attn_out, blend_gain):
    n_st, n_tp = lax.axis_size("st"), lax.axis_size("tp")
    ring = n_st // CORES
    half, xhalf = ring // 2, n_tp // 2
    rows, width = conv.shape[0], mix_out.shape[1]
    mine = rows // n_tp
    blocks = acc.shape[1]
    vmem = pl.BlockSpec(memory_space=pltpu.VMEM)
    return pl.pallas_call(
        functools.partial(blend_kernel, n_st, n_tp),
        out_shape=jax.ShapeDtypeStruct((mine, width), BF16),
        in_specs=[vmem] * 8,
        out_specs=vmem,
        scratch_shapes=[
            pltpu.VMEM((blocks, half, LANES, LANES), BF16),
            pltpu.VMEM((blocks, half, LANES, LANES), BF16),
            pltpu.VMEM((blocks, half, 2, LANES), F32),
            pltpu.VMEM((blocks, half, 2, LANES), F32),
            pltpu.VMEM((1, mine, width), BF16),
            pltpu.VMEM((xhalf, mine, width), BF16),
            pltpu.VMEM((xhalf, mine, width), BF16),
            pltpu.VMEM((blocks, mine, conv.shape[1]), BF16),
            pltpu.VMEM((n_tp,) + sums.shape, F32),
            pltpu.SemaphoreType.DMA((2, blocks, half, 2)),
            pltpu.SemaphoreType.DMA((2, blocks, half, 2)),
            pltpu.SemaphoreType.DMA((2, xhalf, 2)),
            pltpu.SemaphoreType.DMA((2, xhalf, 2)),
            pltpu.SemaphoreType.DMA((n_tp - 1,)),
            pltpu.SemaphoreType.DMA((n_tp - 1,)),
        ],
        compiler_params=pltpu.CompilerParams(
            collective_id=1, has_side_effects=True, vmem_limit_bytes=50 * 2**20
        ),
        name="blend",
    )(acc, stats, conv, sums, channel_gain, mix_out, attn_out, blend_gain)


def rms_rows(row_data, gain_vec):
    floats = row_data.astype(F32)
    inv_scale = lax.rsqrt(jnp.mean(floats * floats, axis=-1, keepdims=True) + EPS)
    return (floats * inv_scale * gain_vec).astype(BF16)


def depthwise(gated_rows, conv_taps):
    span_width = conv_taps.shape[0]
    half_span = (span_width - 1) // 2
    seq_length = gated_rows.shape[1]
    padded = jnp.pad(gated_rows.astype(F32), ((0, 0), (half_span, span_width - 1 - half_span), (0, 0)))
    running = jnp.zeros(gated_rows.shape, F32)
    for tap_index in range(span_width):
        running = running + padded[:, tap_index : tap_index + seq_length] * conv_taps[tap_index].astype(F32)
    return running


def request_tables(passage_ids, chips, chip_passages, slots):
    blocks, per_block = passage_ids.shape
    flat = passage_ids.reshape(-1)
    number = jnp.arange(flat.shape[0])
    chip_of = flat // chip_passages
    local_of = flat - chip_of * chip_passages
    earlier = (chip_of[:, None] == chip_of[None, :]) & (number[None, :] < number[:, None])
    rank = jnp.sum(earlier.astype(jnp.int32), axis=1)
    here = jnp.arange(chips)[:, None] == chip_of[None, :]
    taken = here[:, None, :] & (jnp.arange(slots)[None, :, None] == rank[None, None, :])
    block_of = jnp.sum(jnp.where(taken, number // per_block, 0), axis=2)
    passage_of = jnp.sum(jnp.where(taken, local_of, 0), axis=2)
    slot_of = jnp.where(here, rank, slots)
    table = jnp.concatenate([block_of, passage_of, slot_of], axis=1).astype(jnp.int32)
    return jnp.pad(table, ((0, 0), (0, LANES - table.shape[1])))[:, None, :]


def local(
    tokens, store, passage_ids, mix_gain, glu_value, glu_gate, conv_taps, channel_gain, mix_out,
    query_gain, passage_gain, query_proj, key_proj, value_proj, attn_out, blend_gain,
):
    owners = lax.axis_size("st")
    blocks, per_block = passage_ids.shape
    slots = CORES * (2 * blocks * per_block // owners)
    chips = owners // CORES
    table = request_tables(passage_ids, chips, CORES * store.shape[0], slots)
    acc, stats = serve(
        tokens, store, query_proj, key_proj, value_proj, query_gain[None], passage_gain[None], table,
        slots, blocks, per_block,
    )
    rows, channels = tokens.shape[0], glu_value.shape[1]
    mix_input = rms_rows(tokens, mix_gain)
    value_part = jnp.dot(mix_input, glu_value, preferred_element_type=F32)
    gate_part = jnp.dot(mix_input, glu_gate, preferred_element_type=F32)
    gated_rows = (value_part * jax.nn.sigmoid(gate_part)).astype(BF16)
    conv_rows = depthwise(gated_rows.reshape(-1, SEQ_LEN, channels), conv_taps).reshape(rows, channels)
    sums = jnp.concatenate(
        [jnp.sum(conv_rows, axis=1).reshape(-1, 128), jnp.sum(conv_rows * conv_rows, axis=1).reshape(-1, 128)], axis=0
    )
    return blended_rows(
        acc, stats, conv_rows, sums, channel_gain[None], mix_out, attn_out, blend_gain[None]
    )


def solution(mesh):
    in_specs = (
        P(("grp", "st"), None),
        P(("grp", "st"), None, None),
        P(("grp", "st"), None),
        P(),
        P(None, "tp"),
        P(None, "tp"),
        P(None, "tp"),
        P("tp"),
        P("tp", None),
        P(),
        P(),
        P(None, "tp"),
        P(None, "tp"),
        P(None, "tp"),
        P("tp", None),
        P(),
    )
    out_specs = P(("grp", "st", "tp"), None)
    return jax.shard_map(local, mesh=mesh, in_specs=in_specs, out_specs=out_specs, check_vma=False)
```

```python
import functools

import jax
import jax.numpy as jnp
from jax import lax
from jax.experimental import pallas as pl
from jax.experimental.pallas import tpu as pltpu
from jax.sharding import PartitionSpec as P

CA = 1024
HD = 256
SEQ_LEN = 128
CORES = 2
LANES = 128
EPS = 1e-06
EMPTY = -1e30
BACKLOG = {5: 9.0, 6: 9.0, 7: 1.2, 8: 0.0, 9: 0.0}
MESH = pl.DeviceIdType.MESH
F32 = jnp.float32
BF16 = jnp.bfloat16


def remote(src, dst, send_sem, recv_sem, **target):
    return pltpu.make_async_remote_copy(
        src_ref=src, dst_ref=dst, send_sem=send_sem, recv_sem=recv_sem,
        device_id=target, device_id_type=MESH,
    )


def place_of(distance, n):
    half = n // 2
    return jnp.where(distance >= half, 2 * (distance - half), 2 * (half - distance) - 1)


def order_of(n):
    half = n // 2
    order = [half]
    for j in range(1, half):
        order += [half - j, half + j]
    return order + [0]


def normed_rows(dst, src, gain, rows, step=16, unroll=2):
    @pl.loop(0, rows // step, unroll=unroll)
    def _(i):
        at = pl.ds(pl.multiple_of(i * step, step), step)
        x = src[at, :].astype(F32)
        inv = lax.rsqrt(jnp.mean(x * x, axis=-1, keepdims=True) + EPS)
        dst[at, :] = (x * inv * gain[...]).astype(BF16)


def merged(a, b):
    best = jnp.maximum(a[1], b[1])
    fa, fb = jnp.exp(a[1] - best), jnp.exp(b[1] - best)
    return fa * a[0] + fb * b[0], best, fa * a[2] + fb * b[2]


class Plan:
    def __init__(self):
        self.steps = {}

    def add(self, name, run, time, rank, after=(), gets=(), sends=()):
        self.steps[name] = (run, time, rank, tuple(after), tuple(gets), tuple(sends))

    def order(self, backlog):
        clock, free, arrival, done, order = 0.0, {}, {}, set(), []
        left = list(self.steps)
        while left:
            best = None
            for name in left:
                _, _, rank, after, gets, sends = self.steps[name]
                if all(a in done for a in after) and all(g in arrival for g in gets):
                    ready = max([clock] + [arrival[g] for g in gets])
                    if rank in backlog:
                        ready = max([ready] + [free.get(link, 0.0) - backlog[rank] for _, link, _, _ in sends])
                    if best is None or (ready, rank) < best[0]:
                        best = ((ready, rank), name)
            (ready, _), name = best
            _, time, _, _, _, sends = self.steps[name]
            clock = ready + time
            for message, link, wire, late in sends:
                free[link] = max(free.get(link, 0.0), clock) + wire
                arrival[message] = free[link] + late
            done.add(name)
            left.remove(name)
            order.append((name, ready, clock))
        return order


def step_plan(k):
    plan = Plan()
    ring, half, groups, xhalf = k.ring, k.half, k.groups, k.xhalf
    hop_late, far_late, q_wire, y_wire, x_wire = 2.3, 0.75, 1.4, 0.72, 1.4
    for g in range(groups):
        plan.add(
            ("q", g), functools.partial(k.queries, g), 0.76, 1, [("q", g - 1)] if g else [],
            sends=[(("q", side, 1, g), ("y", side), q_wire, hop_late) for side in range(2)],
        )
    for hop in range(1, half + 1):
        for g in range(groups):
            for side in range(2):
                if hop == half and (g < groups // 2) != (side == 0):
                    continue
                on = hop + 1 < half or (hop + 1 == half and (g < groups // 2) == (side == 0))
                plan.add(
                    ("hand", side, hop, g), functools.partial(k.hand_on, side, hop, g, on), 0.03, 0,
                    gets=[("q", side, hop, g)],
                    sends=[(("q", side, hop + 1, g), ("y", side), q_wire, hop_late)] if on else [],
                )
    pairs = list(range(0, k.passages, 2))
    for p in pairs:
        plan.add(("norm", p), functools.partial(k.norm_passages, p), 0.75, 20, [("v", p - 2)] if p else [("q", groups - 1)])
        plan.add(("k", p), functools.partial(k.keys, p), 0.5, 20, [("norm", p)])
        plan.add(("v", p), functools.partial(k.values, p), 0.65, 20, [("k", p)], sends=[(("kv", p), ("core",), 0.4, 1.0)])
    plan.add(("here",), k.all_here, 0.65, 21, [("v", p) for p in pairs], gets=[("kv", p) for p in pairs])
    for rel in range(ring):
        hop = min(rel, ring - rel)
        if hop == half:
            hands = [("hand", 0 if g < groups // 2 else 1, hop, g) for g in range(groups)]
        elif hop:
            hands = [("hand", 1 if rel < half else 0, hop, g) for g in range(groups)]
        else:
            hands = []
        plan.add(("slots", rel), functools.partial(k.attend, rel), 0.6, 19 - hop, [("here",)] + hands)
        plan.add(("attend", rel), functools.partial(k.join, rel), 0.4, 1, [("slots", rel)])
    for c, chunk in enumerate(k.chunks):
        for p in chunk:
            joined = k.join_side(p)
            if joined is not None:
                plan.add(
                    ("join", p), functools.partial(k.join_late, p), 0.03, 5 + c, [("attend", half)],
                    sends=[(("join", p), ("y", joined), y_wire * (half - k.join_hop(p)),
                            hop_late + far_late * (half - k.join_hop(p) - 1))],
                )
            for side in range(2):
                far = k.start_of(side, p)
                for d in range(far, 0, -1):
                    rel = d if side == 0 else ring - d
                    gets = [] if d == far else [("y", side, p, d)]
                    if joined == side and d == k.join_hop(p):
                        gets = gets + [("join", p)]
                    plan.add(
                        ("y", side, p, d),
                        functools.partial(k.y_start if d == far else k.y_stage, side, p, d), 0.03 if d == far else 0.1,
                        5 + c, [("attend", rel)], gets=gets,
                        sends=[(("y", side, p, d - 1), ("y", side), y_wire, hop_late)],
                    )
    for g in range(groups):
        plan.add(("glu", g), functools.partial(k.glu, g), 0.95, 30, [("q", groups - 1)])
        plan.add(("conv", g), functools.partial(k.convolve, g), 0.25, 29, [("glu", g)])
    plan.add(("sums",), k.send_sums, 0.1, 3, [("conv", g) for g in range(groups)],
             sends=[(("sums",), ("x", 2), 0.5, 5.0)])
    plan.add(("act",), k.activations, 0.4, 4, gets=[("sums",)])
    for c, chunk in enumerate(k.chunks):
        gets = [("y", side, p, 0) for p in chunk for side in range(2)]
        gets += [("join", p) for p in chunk if k.join_side(p) is not None and k.join_hop(p) == 0]
        plan.add(("home", c), functools.partial(k.home, c), 0.3, 4, [("attend", 0)], gets=gets)
        dist = xhalf - c
        for t in range(k.tiles):
            h = t // (k.tiles // 2)
            if dist == xhalf:
                gets, outs = [], [h]
            elif dist == 0:
                gets, outs = [0, 1], []
            else:
                gets = [0, 1] if dist < xhalf - 1 else [h]
                outs = [0, 1]
            plan.add(
                ("project", c, t), functools.partial(k.project, c, t, gets, outs), 0.25, 3, [("home", c), ("act",)],
                gets=[("x", side, dist, t) for side in gets],
                sends=[(("x", side, dist - 1, t), ("x", side), x_wire, hop_late) for side in outs],
            )
    return plan


class Body:
    def __init__(self, n_st, n_tp, slots, blocks, per_block, refs):
        self.__dict__.update(refs)
        self.n_st, self.n_tp, self.slots, self.blocks, self.per_block = n_st, n_tp, slots, blocks, per_block
        self.ring, self.groups = n_st // CORES, self.tok_hbm.shape[0] // 128
        self.half, self.xhalf = self.ring // 2, n_tp // 2
        self.passages = self.store_hbm.shape[0]
        self.per_group = blocks // self.groups
        self.block_len = 128 // self.per_group
        self.width = self.tok_hbm.shape[1]
        self.tile = 512
        self.tiles = self.width // self.tile
        self.me, self.x_me = lax.axis_index("st"), lax.axis_index("tp")
        self.core, self.y_me = lax.rem(self.me, CORES), self.me // CORES
        self.partner = self.me + 1 - 2 * self.core
        self.right, self.left = self.chip(1), self.chip(self.ring - 1)
        self.sends, self.loads = [], []
        self.early = 2
        self.places = order_of(n_tp)
        self.chunks = [[0]] + [[2 * j - 1, 2 * j] for j in range(1, self.xhalf)] + [[n_tp - 1]]
        self.start_cw = {}
        for c, chunk in enumerate(self.chunks):
            for i, p in enumerate(chunk):
                self.start_cw[p] = self.half if (i == 0 and c < len(self.chunks) - 1) else self.half - 1

    def chip(self, d):
        return lax.rem(self.me + CORES * d, self.n_st)

    def column(self, d):
        return lax.rem(self.x_me + d, self.n_tp)

    def send(self, copy):
        copy.start()
        self.sends.append(copy)

    def load(self, src, dst):
        copy = pltpu.make_async_copy(src, dst, self.load_sem.at[len(self.loads)])
        copy.start()
        self.loads.append(copy)
        return copy

    def start_of(self, side, p):
        if self.join_side(p) is not None:
            return self.half - 1
        return self.start_cw[p] if side == 0 else 2 * self.half - 1 - self.start_cw[p]

    def enter(self):
        small = lambda name: self.load(getattr(self, name + "_hbm"), getattr(self, name))
        self.first_loads = [small("qgain"), self.load(self.wq_hbm, self.wq)]
        rows = lambda g: pl.ds(g * 128, 128)
        self.tok_loads = [self.load(self.tok_hbm.at[rows(g)], self.tok.at[rows(g)]) for g in range(self.groups)]
        self.table_load = small("table")
        self.kv_loads = [small("pgain"), self.load(self.wk_hbm, self.wk), self.load(self.wv_hbm, self.wv)]
        self.store_loads = [
            self.load(self.store_hbm.at[p], self.store.at[pl.ds(p * 128, 128)]) for p in range(self.passages)
        ]
        self.glu_loads = [
            small("mgain"), small("taps"), small("cgain"),
            self.load(self.gv_hbm, self.wglu.at[:, pl.ds(0, LANES)]),
            self.load(self.gg_hbm, self.wglu.at[:, pl.ds(LANES, LANES)]),
        ]
        self.out_loads = [small("blend"), self.load(self.attn_hbm, self.attn), self.load(self.mix_hbm, self.mix)]
        barrier = pltpu.get_barrier_semaphore()
        for d in range(1, self.ring):
            pl.semaphore_signal(barrier, inc=1, device_id={"st": self.chip(d)}, device_id_type=MESH)
        pl.semaphore_signal(barrier, inc=1, device_id={"st": self.partner}, device_id_type=MESH)
        for d in range(1, self.n_tp):
            pl.semaphore_signal(barrier, inc=1, device_id={"tp": self.column(d)}, device_id_type=MESH)
        s = self.slots
        self.outs[s] = jnp.zeros(self.outs.shape[1:], BF16)
        self.ml[s, 0:1] = jnp.full((1, LANES), EMPTY, F32)
        self.ml[s, 1:2] = jnp.zeros((1, LANES), F32)
        self.padded[...] = jnp.zeros(self.padded.shape, F32)

    def entered(self):
        self.table_load.wait()
        pl.semaphore_wait(pltpu.get_barrier_semaphore(), self.ring + self.n_tp - 1)
        for d in range(1, self.ring):
            self.send(remote(self.table.at[lax.rem(self.y_me + d, self.ring)], self.tabv.at[self.ring - d],
                             self.t_send.at[d - 1], self.t_recv.at[self.ring - d - 1], st=self.chip(d)))
        self.own_table = pltpu.make_async_copy(self.table.at[self.y_me], self.tabv.at[0], self.s_sem.at[1])
        self.own_table.start()


    def part(self, rel, g):
        return self.qall[rel].at[pl.ds(self.per_group * g, self.per_group)]

    def queries(self, g):
        self.tok_loads[g].wait()
        if g == 0:
            self.first_loads[0].wait()
        normed_rows(self.xn.at[pl.ds(0, 128)], self.tok.at[pl.ds(g * 128, 128)], self.qgain, 128, unroll=4)
        if g == 0:
            self.first_loads[1].wait()
        q = jnp.dot(self.xn[pl.ds(0, 128), :], self.wq[...], preferred_element_type=F32).astype(BF16)
        n = self.block_len
        for i in range(self.per_group):
            self.qall[0][self.per_group * g + i] = q[i * n : (i + 1) * n]
        if g == 0:
            with jax.named_scope("entry"):
                self.entered()
        for side, rel, who in ((0, self.ring - 1, self.right), (1, 1, self.left)):
            self.send(remote(self.part(0, g), self.part(rel, g), self.q_send.at[side, 0, g], self.q_recv.at[side, 0, g],
                             st=who))

    def hand_on(self, side, hop, g, on):
        rel = self.ring - hop if side == 0 else hop
        here = self.part(rel, g)
        remote(here, here, self.q_send.at[side, hop - 1, g], self.q_recv.at[side, hop - 1, g], st=self.right).wait_recv()
        if on:
            there = self.part(rel - 1 if side == 0 else rel + 1, g)
            self.send(remote(here, there, self.q_send.at[side, hop, g], self.q_recv.at[side, hop, g],
                             st=self.right if side == 0 else self.left))


    def norm_passages(self, p):
        for i in range(2):
            self.store_loads[p + i].wait()
        if p == 0:
            for copy in self.kv_loads:
                copy.wait()
        normed_rows(self.xn, self.store.at[pl.ds(p * 128, 256)], self.pgain, 256)

    def share(self, j, ref, at, p):
        self.send(remote(ref.at[at], ref.at[at], self.kv_send.at[j, p], self.kv_recv.at[j, p], st=self.partner))

    def keys(self, p):
        k = jnp.dot(self.xn[...], self.wk[...], preferred_element_type=F32).astype(BF16)
        for i in range(2):
            at = self.core * self.passages + p + i
            self.kall[at] = k[i * 128 : (i + 1) * 128]
            self.share(0, self.kall, at, p + i)

    def values(self, p):
        v = jnp.dot(self.xn[...], self.wv[...], preferred_element_type=F32)
        for i in range(2):
            at = self.core * self.passages + p + i
            w = v[i * 128 : (i + 1) * 128]
            self.vall[at] = jnp.concatenate([w[:, :LANES].T, w[:, LANES:].T], axis=1).astype(BF16)
            self.share(1, self.vall, at, p + i)

    def all_here(self):
        for p in range(self.passages):
            other = (1 - self.core) * self.passages + p
            for j, ref in enumerate((self.kall, self.vall)):
                remote(ref.at[other], ref.at[other], self.kv_send.at[j, p], self.kv_recv.at[j, p],
                       st=self.partner).wait_recv()
        self.own_table.wait()
        for d in range(1, self.ring):
            here = self.tabv.at[d]
            remote(here, here, self.t_send.at[d - 1], self.t_recv.at[d - 1], st=self.partner).wait_recv()
        to_scalar = pltpu.make_async_copy(self.tabv, self.tabs, self.s_sem.at[0])
        to_scalar.start()
        to_scalar.wait()


    def attend(self, rel):
        low_half = lax.broadcasted_iota(jnp.int32, (LANES, LANES), 1) < LANES // 2
        slots, tabs, ml, outs = self.slots, self.tabs, self.ml, self.outs
        for k in range(slots):
            q = self.qall[rel][tabs[rel, 0, k]]
            p = tabs[rel, 0, slots + k]
            s = lax.dot_general(
                self.kall[p], jnp.concatenate([q, q], axis=0), (((1,), (1,)), ((), ())), preferred_element_type=F32
            ) * HD ** (-0.5)
            top = jnp.max(s, axis=0, keepdims=True)
            e = jnp.exp(s - top)
            ml[k, 0:1] = top
            ml[k, 1:2] = jnp.sum(e, axis=0, keepdims=True)
            w = jnp.concatenate([jnp.where(low_half, e, 0.0), jnp.where(low_half, 0.0, e)], axis=0).astype(BF16)
            outs[k] = jnp.dot(self.vall[p], w, preferred_element_type=F32).astype(BF16)

    def join(self, rel):
        slots, tabs, ml, outs = self.slots, self.tabs, self.ml, self.outs

        @pl.loop(0, self.blocks)
        def _(distance):
            b = lax.rem(self.x_me + distance, self.blocks)
            at = [tabs[rel, 0, 2 * slots + b * self.per_block + j] for j in range(self.per_block)]
            mls = [ml[i] for i in at]
            best = functools.reduce(jnp.maximum, [a[0:1] for a in mls])
            scale = [jnp.exp(a[0:1] - best) for a in mls]
            total = sum(f * a[1:2] for f, a in zip(scale, mls))
            num = sum(f * outs[i].astype(F32) for f, i in zip(scale, at))
            place = place_of(distance, self.n_tp)
            self.acc[rel, place] = num.astype(BF16)
            self.stats[rel, place, 0:1] = best
            self.stats[rel, place, 1:2] = total


    def y_out(self, side, p, d, num, stat):
        who = self.right if side == 0 else self.left
        for i, (src, dst) in enumerate(((num, self.ydata), (stat, self.ystat))):
            self.send(remote(src, dst.at[side, p, d - 1], self.y_send.at[side, p, d - 1, i],
                             self.y_recv.at[side, p, d - 1, i], st=who))

    def y_start(self, side, p, d):
        rel = d if side == 0 else self.ring - d
        self.y_out(side, p, d, self.acc.at[rel, p], self.stats.at[rel, p])

    def y_arrived(self, side, p, d):
        for i, ref in enumerate((self.ydata, self.ystat)):
            here = ref.at[side, p, d]
            remote(here, here, self.y_send.at[side, p, d, i], self.y_recv.at[side, p, d, i], st=self.right).wait_recv()
        stat = self.ystat.at[side, p, d]
        return self.ydata[side, p, d].astype(F32), stat[0:1], stat[1:2]

    def own(self, rel, p):
        return self.acc[rel, p].astype(F32), self.stats[rel, p, 0:1], self.stats[rel, p, 1:2]

    def y_stage(self, side, p, d):
        so_far = merged(self.y_arrived(side, p, d), self.own(d if side == 0 else self.ring - d, p))
        if self.join_side(p) == side and self.join_hop(p) == d:
            so_far = merged(so_far, self.joined(p))
        num, best, total = so_far
        self.ydata[side, p, d] = num.astype(BF16)
        self.ystat[side, p, d, 0:1] = best
        self.ystat[side, p, d, 1:2] = total
        self.y_out(side, p, d, self.ydata.at[side, p, d], self.ystat.at[side, p, d])

    def join_side(self, p):
        early = [q for chunk in self.chunks[: self.early] for q in chunk]
        return (early.index(p) + 1) % 2 if p in early else None

    def join_hop(self, p):
        return 0 if p == self.chunks[0][0] else 1

    def join_late(self, p):
        side = self.join_side(p)
        hops = self.half - self.join_hop(p)
        who = self.chip(hops if side == 0 else self.ring - hops)
        for i, (src, dst) in enumerate(((self.acc, self.jdata), (self.stats, self.jstat))):
            self.send(remote(src.at[self.half, p], dst.at[p], self.j_send.at[p, i], self.j_recv.at[p, i], st=who))

    def joined(self, p):
        for i, ref in enumerate((self.jdata, self.jstat)):
            here = ref.at[p]
            remote(here, here, self.j_send.at[p, i], self.j_recv.at[p, i], st=self.right).wait_recv()
        stat = self.jstat.at[p]
        return self.jdata[p].astype(F32), stat[0:1], stat[1:2]

    def home(self, c):
        for i, p in enumerate(self.chunks[c]):
            so_far = merged(merged(self.y_arrived(0, p, 0), self.own(0, p)), self.y_arrived(1, p, 0))
            if self.join_side(p) is not None and self.join_hop(p) == 0:
                so_far = merged(so_far, self.joined(p))
            num, best, total = so_far
            t = (num / total).T.astype(BF16)
            n = self.block_len
            self.rows_a[c, pl.ds(i * n, n), :] = jnp.concatenate([t[:n], t[n:]], axis=1)


    def glu(self, g):
        xm = self.xm
        if g == 0:
            for copy in self.glu_loads:
                copy.wait()
        normed_rows(xm, self.tok.at[pl.ds(g * 128, 128)], self.mgain, 128)
        y = jnp.dot(xm[...], self.wglu[...], preferred_element_type=F32)
        gated = y[:, :LANES] * jax.nn.sigmoid(y[:, LANES:])
        self.padded[g, pl.ds(16, 128), :] = gated.astype(BF16).astype(F32)

    def convolve(self, g):
        taps = self.taps[...].astype(F32)
        span = taps.shape[0]
        first = 16 - (span - 1) // 2
        running = jnp.zeros((128, LANES), F32)
        for k in range(span):
            running = running + self.padded[g, pl.ds(first + k, 128), :] * taps[k : k + 1]
        self.conv[g] = running
        turned = running.T
        self.sums[g : g + 1, :] = jnp.sum(turned, axis=0, keepdims=True)
        at = self.groups + g
        self.sums[at : at + 1, :] = jnp.sum(turned * turned, axis=0, keepdims=True)

    def send_sums(self):
        for d in range(1, self.n_tp):
            self.send(remote(self.sums, self.allsums.at[self.n_tp - d], self.c_send.at[d - 1],
                             self.c_recv.at[self.n_tp - d - 1], tp=self.column(d)))

    def activations(self):
        total = self.sums[...]
        for d in range(1, self.n_tp):
            here = self.allsums.at[d]
            remote(here, here, self.c_send.at[d - 1], self.c_recv.at[d - 1], tp=self.column(1)).wait_recv()
            total = total + self.allsums[d]
        groups = self.groups
        mean = total[:groups] / CA
        var = total[groups:] / CA - mean * mean
        cols = jnp.concatenate([mean, lax.rsqrt(var + EPS)], axis=0).T
        n = self.block_len
        for g in range(groups):
            z = (self.conv[g] - cols[:, g : g + 1]) * cols[:, groups + g : groups + g + 1] * self.cgain[...]
            z = (z / (1.0 + jnp.exp(-z))).astype(BF16)
            for i in range(self.per_group):
                self.act[g * self.per_group + i] = z[i * n : (i + 1) * n]


    def project(self, c, t, gets, outs):
        chunk, k, n = self.chunks[c], self.xhalf - c, self.block_len
        at = pl.ds(t * self.tile, self.tile)
        if c == 0 and t == 0:
            for copy in self.out_loads:
                copy.wait()
        rows_p = jnp.concatenate([self.act[self.column(self.places[p])] for p in chunk], axis=0)
        y = jnp.dot(rows_p, self.mix[:, at], preferred_element_type=F32) + self.blend[:, at] * jnp.dot(
            self.rows_a[c, pl.ds(0, n * len(chunk)), :], self.attn[:, at], preferred_element_type=F32
        )
        for side in gets:
            here = self.xdata.at[side, k, t]
            remote(here, here, self.x_send.at[side, k, t], self.x_recv.at[side, k, t], tp=self.column(1)).wait_recv()
        if k == 0:
            y = y + self.xdata[0, k, t].astype(F32) + self.xdata[1, k, t].astype(F32)
            self.out[:, at] = y.astype(BF16)
            return
        for side in outs:
            mine = y if len(chunk) == 1 else y[side * n : (side + 1) * n]
            if side in gets:
                mine = mine + self.xdata[side, k, t].astype(F32)
            slot = self.xdata.at[side, k, t] if k < self.xhalf else self.xfirst.at[t]
            slot[...] = mine.astype(BF16)
            self.send(remote(slot, self.xdata.at[side, k - 1, t], self.x_send.at[side, k - 1, t],
                             self.x_recv.at[side, k - 1, t],
                             tp=self.column(1 if side == 0 else self.n_tp - 1)))


def whole_kernel(names, n_st, n_tp, slots, blocks, per_block, *refs):
    ring = n_st // CORES
    at = names.index("qall")
    found = dict(zip(names[:at] + names[at + 1 :], refs[:at] + refs[at + ring :]))
    found["qall"] = refs[at : at + ring]
    k = Body(n_st, n_tp, slots, blocks, per_block, found)
    plan = step_plan(k)
    with jax.named_scope("enter"):
        k.enter()
    for name, _, _ in plan.order(BACKLOG):
        with jax.named_scope("_".join(str(part) for part in name)):
            plan.steps[name][0]()
    for copy in k.sends:
        copy.wait_send()


def whole(table, slots, blocks, per_block, big, small):
    n_st, n_tp = lax.axis_size("st"), lax.axis_size("tp")
    ring, half, xhalf = n_st // CORES, n_st // CORES // 2, n_tp // 2
    rows, width = big["tok_hbm"].shape
    passages, prows, _ = big["store_hbm"].shape
    groups, block_len, mine = rows // 128, rows // blocks, rows // n_tp
    channels = big["gv_hbm"].shape[1]
    assert prows == 128 and big["wq_hbm"].shape[1] == HD and channels == LANES
    assert block_len * 2 == LANES and blocks == n_tp and passages % 2 == 0
    tiles = width // 512
    dma = pltpu.SemaphoreType.DMA
    scratch = {
        "tok": pltpu.VMEM((rows, width), BF16),
        "store": pltpu.VMEM((passages * prows, width), BF16),
        "wq": pltpu.VMEM((width, HD), BF16),
        "wk": pltpu.VMEM((width, HD), BF16),
        "wv": pltpu.VMEM((width, HD), BF16),
        "wglu": pltpu.VMEM((width, 2 * LANES), BF16),
        "attn": pltpu.VMEM((HD, width), BF16),
        "mix": pltpu.VMEM((channels, width), BF16),
        "xn": pltpu.VMEM((256, width), BF16),
        "xm": pltpu.VMEM((128, width), BF16),
        "kall": pltpu.VMEM((CORES * passages, prows, HD), BF16),
        "vall": pltpu.VMEM((CORES * passages, LANES, 2 * prows), BF16),
        "outs": pltpu.VMEM((slots + 1, LANES, LANES), BF16),
        "ml": pltpu.VMEM((slots + 1, 2, LANES), F32),
        "tabv": pltpu.VMEM(table.shape, jnp.int32),
        "tabs": pltpu.SMEM(table.shape, jnp.int32),
        "acc": pltpu.VMEM((ring, blocks, LANES, LANES), BF16),
        "stats": pltpu.VMEM((ring, blocks, 2, LANES), F32),
        "ydata": pltpu.VMEM((2, blocks, half, LANES, LANES), BF16),
        "ystat": pltpu.VMEM((2, blocks, half, 2, LANES), F32),
        "jdata": pltpu.VMEM((blocks, LANES, LANES), BF16),
        "jstat": pltpu.VMEM((blocks, 2, LANES), F32),
        "rows_a": pltpu.VMEM((xhalf + 1, 2 * block_len, HD), BF16),
        "padded": pltpu.VMEM((groups, 128 + 32, LANES), F32),
        "conv": pltpu.VMEM((groups, 128, LANES), F32),
        "sums": pltpu.VMEM((2 * groups, 128), F32),
        "allsums": pltpu.VMEM((n_tp, 2 * groups, 128), F32),
        "act": pltpu.VMEM((blocks, block_len, channels), BF16),
        "xdata": pltpu.VMEM((2, xhalf, tiles, mine, 512), BF16),
        "xfirst": pltpu.VMEM((tiles, mine, 512), BF16),
        "load_sem": dma((7 + groups + passages + len(small) + 1,)),
        "q_send": dma((2, half, groups)),
        "q_recv": dma((2, half, groups)),
        "kv_send": dma((2, passages)),
        "kv_recv": dma((2, passages)),
        "t_send": dma((ring - 1,)),
        "t_recv": dma((ring - 1,)),
        "s_sem": dma((2,)),
        "y_send": dma((2, blocks, half, 2)),
        "y_recv": dma((2, blocks, half, 2)),
        "j_send": dma((blocks, 2)),
        "j_recv": dma((blocks, 2)),
        "x_send": dma((2, xhalf, tiles)),
        "x_recv": dma((2, xhalf, tiles)),
        "c_send": dma((n_tp - 1,)),
        "c_recv": dma((n_tp - 1,)),
        "qall": None,
    }
    scratch = {**{n[:-4]: pltpu.VMEM(a.shape, a.dtype) for n, a in small.items()},
               "table": pltpu.VMEM(table.shape, table.dtype), **scratch}
    names = list(big) + list(small) + ["table_hbm", "out"] + list(scratch)
    shapes = [s for n, s in scratch.items() if n != "qall"]
    shapes += [pltpu.VMEM((blocks, block_len, HD), BF16) for _ in range(ring)]
    vmem = pl.BlockSpec(memory_space=pltpu.VMEM)
    return pl.pallas_call(
        functools.partial(whole_kernel, names, n_st, n_tp, slots, blocks, per_block),
        out_shape=jax.ShapeDtypeStruct((mine, width), BF16),
        in_specs=[pl.BlockSpec(memory_space=pl.ANY)] * (len(big) + len(small) + 1),
        out_specs=vmem,
        scratch_shapes=shapes,
        compiler_params=pltpu.CompilerParams(
            collective_id=0, has_side_effects=True, vmem_limit_bytes=66_000_000
        ),
        name="whole",
    )(*big.values(), *small.values(), table)


def request_tables(passage_ids, chips, chip_passages, slots):
    blocks, per_block = passage_ids.shape
    flat = passage_ids.reshape(-1)
    number = jnp.arange(flat.shape[0])
    chip_of = flat // chip_passages
    local_of = flat - chip_of * chip_passages
    earlier = (chip_of[:, None] == chip_of[None, :]) & (number[None, :] < number[:, None])
    rank = jnp.sum(earlier.astype(jnp.int32), axis=1)
    here = jnp.arange(chips)[:, None] == chip_of[None, :]
    taken = here[:, None, :] & (jnp.arange(slots)[None, :, None] == rank[None, None, :])
    block_of = jnp.sum(jnp.where(taken, number // per_block, 0), axis=2)
    passage_of = jnp.sum(jnp.where(taken, local_of, 0), axis=2)
    slot_of = jnp.where(here, rank, slots)
    table = jnp.concatenate([block_of, passage_of, slot_of], axis=1).astype(jnp.int32)
    return jnp.pad(table, ((0, 0), (0, LANES - table.shape[1])))[:, None, :]


def local(
    tokens, store, passage_ids, mix_gain, glu_value, glu_gate, conv_taps, channel_gain, mix_out,
    query_gain, passage_gain, query_proj, key_proj, value_proj, attn_out, blend_gain,
):
    owners = lax.axis_size("st")
    blocks, per_block = passage_ids.shape
    slots = CORES * (2 * blocks * per_block // owners)
    table = request_tables(passage_ids, owners // CORES, CORES * store.shape[0], slots)
    big = {
        "tok_hbm": tokens, "store_hbm": store, "wq_hbm": query_proj, "wk_hbm": key_proj, "wv_hbm": value_proj,
        "gv_hbm": glu_value, "gg_hbm": glu_gate, "attn_hbm": attn_out, "mix_hbm": mix_out,
    }
    small = {
        "qgain_hbm": query_gain[None], "pgain_hbm": passage_gain[None], "mgain_hbm": mix_gain[None], "taps_hbm": conv_taps,
        "cgain_hbm": channel_gain[None], "blend_hbm": blend_gain[None],
    }
    return whole(table, slots, blocks, per_block, big, small)


def solution(mesh):
    in_specs = (
        P(("grp", "st"), None),
        P(("grp", "st"), None, None),
        P(("grp", "st"), None),
        P(),
        P(None, "tp"),
        P(None, "tp"),
        P(None, "tp"),
        P("tp"),
        P("tp", None),
        P(),
        P(),
        P(None, "tp"),
        P(None, "tp"),
        P(None, "tp"),
        P("tp", None),
        P(),
    )
    out_specs = P(("grp", "st", "tp"), None)
    return jax.shard_map(local, mesh=mesh, in_specs=in_specs, out_specs=out_specs, check_vma=False)
```

```python
import functools

import jax
import jax.numpy as jnp
from jax import lax
from jax.experimental import pallas as pl
from jax.experimental.pallas import tpu as pltpu
from jax.sharding import PartitionSpec as P

CA = 1024
HD = 256
SEQ_LEN = 128
CORES = 2
LANES = 128
EPS = 1e-06
EMPTY = -1e30
BACKLOG = {6: 9.0, 7: 0.8, 8: 0.15, 9: 0.15}
MESH = pl.DeviceIdType.MESH
F32 = jnp.float32
BF16 = jnp.bfloat16


def remote(src, dst, send_sem, recv_sem, **target):
    return pltpu.make_async_remote_copy(
        src_ref=src, dst_ref=dst, send_sem=send_sem, recv_sem=recv_sem,
        device_id=target, device_id_type=MESH,
    )


def place_of(distance, n):
    half = n // 2
    return jnp.where(distance >= half, 2 * (distance - half), 2 * (half - distance) - 1)


def order_of(n):
    half = n // 2
    order = [half]
    for j in range(1, half):
        order += [half - j, half + j]
    return order + [0]


def normed_rows(dst, src, gain, rows, step=16, unroll=2):
    @pl.loop(0, rows // step, unroll=unroll)
    def _(i):
        at = pl.ds(pl.multiple_of(i * step, step), step)
        x = src[at, :].astype(F32)
        inv = lax.rsqrt(jnp.mean(x * x, axis=-1, keepdims=True) + EPS)
        dst[at, :] = (x * inv * gain[...]).astype(BF16)


def merged(a, b):
    best = jnp.maximum(a[1], b[1])
    fa, fb = jnp.exp(a[1] - best), jnp.exp(b[1] - best)
    return fa * a[0] + fb * b[0], best, fa * a[2] + fb * b[2]


class Plan:
    def __init__(self):
        self.steps = {}

    def add(self, name, run, time, rank, after=(), gets=(), sends=()):
        self.steps[name] = (run, time, rank, tuple(after), tuple(gets), tuple(sends))

    def order(self, backlog):
        clock, free, arrival, done, order = 0.0, {}, {}, set(), []
        left = list(self.steps)
        while left:
            best = None
            for name in left:
                _, _, rank, after, gets, sends = self.steps[name]
                if all(a in done for a in after) and all(g in arrival for g in gets):
                    ready = max([clock] + [arrival[g] for g in gets])
                    if rank in backlog:
                        ready = max([ready] + [free.get(link, 0.0) - backlog[rank] for _, link, *_ in sends])
                    if best is None or (ready, rank) < best[0]:
                        best = ((ready, rank), name)
            (ready, _), name = best
            _, time, _, _, _, sends = self.steps[name]
            clock = ready + time
            for message, link, wire, late, *hops in sends:
                free[link] = max(free.get(link, 0.0), clock) + wire
                arrival[message] = free[link] + late
                free[link] += wire * (hops[0] - 1 if hops else 0)
            done.add(name)
            left.remove(name)
            order.append((name, ready, clock))
        return order


def step_plan(k):
    plan = Plan()
    ring, half, groups, xhalf = k.ring, k.half, k.groups, k.xhalf
    hop_late, far_late, q_wire, y_wire, x_wire = 2.4, 0.75, 1.4, 0.72, 1.4
    for g in range(groups):
        plan.add(
            ("q", g), functools.partial(k.queries, g), 0.76, 1, [("q", g - 1)] if g else [],
            sends=[(("q", side, 1, g), ("y", side), q_wire, hop_late) for side in range(2)],
        )
    for hop in range(1, half + 1):
        for g in range(groups):
            for side in range(2):
                if hop == half and (g < groups // 2) != (side == 0):
                    continue
                on = hop + 1 < half or (hop + 1 == half and (g < groups // 2) == (side == 0))
                plan.add(
                    ("hand", side, hop, g), functools.partial(k.hand_on, side, hop, g, on), 0.03, 0,
                    gets=[("q", side, hop, g)],
                    sends=[(("q", side, hop + 1, g), ("y", side), q_wire, hop_late)] if on else [],
                )
    pairs = list(range(0, k.passages, 2))
    for p in pairs:
        if p == 0:
            plan.add(("norm", p), functools.partial(k.norm_passages, p), 1.0, 20, [("q", groups - 1)])
        plan.add(("k", p), functools.partial(k.keys, p), 0.77, 20, [("v", p - 2) if p else ("norm", p)])
        plan.add(("v", p), functools.partial(k.values, p), 0.86, 20, [("k", p)], sends=[(("kv", p), ("core",), 0.4, 1.0)])
    plan.add(("here",), k.all_here, 0.65, 21, [("v", p) for p in pairs], gets=[("kv", p) for p in pairs])
    for rel in range(ring):
        hop = min(rel, ring - rel)
        if hop == half:
            hands = [("hand", 0 if g < groups // 2 else 1, hop, g) for g in range(groups)]
        elif hop:
            hands = [("hand", 1 if rel < half else 0, hop, g) for g in range(groups)]
        else:
            hands = []
        plan.add(("slots", rel), functools.partial(k.attend, rel), 0.6, 19 - hop, [("here",)] + hands)
        plan.add(("attend", rel), functools.partial(k.join, rel), 0.3, 1, [("slots", rel)])
    for rel in range(1, ring):
        hop = min(rel, ring - rel)
        plan.add(
            ("direct", rel), functools.partial(k.direct, rel), 0.04, 2, [("attend", rel)],
            sends=[(("direct", ring - rel), ("y", 0 if rel <= half else 1), y_wire, hop_late + far_late * (hop - 1), hop)],
        )
    for c, chunk in enumerate(k.chunks[1:], 1):
        for p in chunk:
            joined = k.join_side(p)
            if joined is not None:
                plan.add(
                    ("join", p), functools.partial(k.join_late, p), 0.04, 5 + c, [("attend", half)],
                    sends=[(("join", p), ("y", joined), y_wire, hop_late + far_late * (half - 2), half - 1)],
                )
            for side in range(2):
                far = k.start_of(side, p)
                for d in range(far, 0, -1):
                    rel = d if side == 0 else ring - d
                    gets = [] if d == far else [("y", side, p, d)]
                    if joined == side and d == 1:
                        gets = gets + [("join", p)]
                    plan.add(
                        ("y", side, p, d),
                        functools.partial(k.y_start if d == far else k.y_stage, side, p, d), 0.04 if d == far else 0.06,
                        5 + c, [("attend", rel)], gets=gets,
                        sends=[(("y", side, p, d - 1), ("y", side), y_wire, hop_late)],
                    )
    for g in range(groups):
        plan.add(("glu", g), functools.partial(k.glu, g), 0.95, 30, [("q", groups - 1)])
        plan.add(("conv", g), functools.partial(k.convolve, g), 0.25, 29, [("glu", g)])
    plan.add(("sums",), k.send_sums, 0.1, 3, [("conv", g) for g in range(groups)],
             sends=[(("sums",), ("x", 2), 0.5, 5.0)])
    plan.add(("act",), k.activations, 0.4, 4, gets=[("sums",)])
    for c, chunk in enumerate(k.chunks):
        if c == 0:
            gets = [("direct", rel) for rel in range(1, ring)]
        else:
            gets = [("y", side, p, 0) for p in chunk for side in range(2)]
        plan.add(("home", c), functools.partial(k.home, c), 0.3, 4, [("attend", 0)], gets=gets)
        dist = xhalf - c
        for t in range(k.tiles):
            h = t // (k.tiles // 2)
            if dist == xhalf:
                gets, outs = [], [h]
            elif dist == 0:
                gets, outs = [0, 1], []
            else:
                gets = [0, 1] if dist < xhalf - 1 else [h]
                outs = [0, 1]
            plan.add(
                ("project", c, t), functools.partial(k.project, c, t, gets, outs), 0.25, 3, [("home", c), ("act",)],
                gets=[("x", side, dist, t) for side in gets],
                sends=[(("x", side, dist - 1, t), ("x", side), x_wire, hop_late) for side in outs],
            )
    return plan


class Body:
    def __init__(self, n_st, n_tp, slots, blocks, per_block, refs):
        self.__dict__.update(refs)
        self.n_st, self.n_tp, self.slots, self.blocks, self.per_block = n_st, n_tp, slots, blocks, per_block
        self.ring, self.groups = n_st // CORES, self.tok_hbm.shape[0] // 128
        self.half, self.xhalf = self.ring // 2, n_tp // 2
        self.passages = self.store_hbm.shape[0]
        self.per_group = blocks // self.groups
        self.block_len = 128 // self.per_group
        self.width = self.tok_hbm.shape[1]
        self.tile = 512
        self.tiles = self.width // self.tile
        self.me, self.x_me = lax.axis_index("st"), lax.axis_index("tp")
        self.core, self.y_me = lax.rem(self.me, CORES), self.me // CORES
        self.partner = self.me + 1 - 2 * self.core
        self.right, self.left = self.chip(1), self.chip(self.ring - 1)
        self.waiting, self.unused, self.loads, self.clock = [], list(range(refs["send_sem"].shape[0])), [], 0.0
        self.early = 2
        self.places = order_of(n_tp)
        self.chunks = [[0]] + [[2 * j - 1, 2 * j] for j in range(1, self.xhalf)] + [[n_tp - 1]]
        self.start_cw = {}
        for c, chunk in enumerate(self.chunks):
            for i, p in enumerate(chunk):
                self.start_cw[p] = self.half if (i == 0 and c < len(self.chunks) - 1) else self.half - 1

    def chip(self, d):
        return lax.rem(self.me + CORES * d, self.n_st)

    def column(self, d):
        return lax.rem(self.x_me + d, self.n_tp)

    def send(self, src, dst, recv_sem, **target):
        self.send_all([(src, dst)], recv_sem, **target)

    def send_all(self, pairs, recv_sem, **target):
        if not self.unused:
            self.settle()
        at = self.unused.pop(0)
        sem = self.send_sem.at[at]
        for src, dst in pairs:
            remote(src, dst, sem, recv_sem, **target).start()
        whole = self.both if len(pairs) > 1 else pairs[0][0]
        self.waiting.append((self.clock, remote(whole, whole, sem, recv_sem, **target), at))

    def settle(self):
        _, copy, at = self.waiting.pop(0)
        copy.wait_send()
        self.unused.append(at)

    def got(self, ref, recv_sem):
        remote(ref, ref, self.send_sem.at[0], recv_sem, st=self.partner).wait_recv()

    def load(self, src, dst):
        copy = pltpu.make_async_copy(src, dst, self.load_sem.at[len(self.loads)])
        copy.start()
        self.loads.append(copy)
        return copy

    def start_of(self, side, p):
        if self.join_side(p) is not None:
            return self.half - 1
        return self.start_cw[p] if side == 0 else 2 * self.half - 1 - self.start_cw[p]

    def enter(self):
        small = lambda name: self.load(getattr(self, name + "_hbm"), getattr(self, name))
        self.first_loads = [small("qgain"), self.load(self.wq_hbm, self.wq)]
        rows = lambda g: pl.ds(g * 128, 128)
        self.tok_loads = [self.load(self.tok_hbm.at[rows(g)], self.tok.at[rows(g)]) for g in range(self.groups)]
        self.ids_load = small("ids")
        self.kv_loads = [small("pgain"), self.load(self.wk_hbm, self.wk), self.load(self.wv_hbm, self.wv)]
        self.store_loads = [
            self.load(self.store_hbm.at[p], self.store.at[pl.ds(p * 128, 128)]) for p in range(self.passages)
        ]
        self.glu_loads = [
            small("mgain"), small("taps"), small("cgain"),
            self.load(self.gv_hbm, self.wglu.at[:, pl.ds(0, LANES)]),
            self.load(self.gg_hbm, self.wglu.at[:, pl.ds(LANES, LANES)]),
        ]
        self.out_loads = [small("blend"), self.load(self.attn_hbm, self.attn), self.load(self.mix_hbm, self.mix)]
        barrier = pltpu.get_barrier_semaphore()
        for d in range(1, self.ring):
            pl.semaphore_signal(barrier, inc=1, device_id={"st": self.chip(d)}, device_id_type=MESH)
        pl.semaphore_signal(barrier, inc=1, device_id={"st": self.partner}, device_id_type=MESH)
        for d in range(1, self.n_tp):
            pl.semaphore_signal(barrier, inc=1, device_id={"tp": self.column(d)}, device_id_type=MESH)
        s = self.slots
        self.outs[s] = jnp.zeros(self.outs.shape[1:], BF16)
        self.ml[s, 0:1] = jnp.full((1, LANES), EMPTY, F32)
        self.ml[s, 1:2] = jnp.zeros((1, LANES), F32)
        self.padded[...] = jnp.zeros(self.padded.shape, F32)

    def make_table(self):
        self.ids_load.wait()
        chip = lax.broadcasted_iota(jnp.int32, (self.ring, LANES), 0)
        lane = lax.broadcasted_iota(jnp.int32, (self.ring, LANES), 1)
        used = jnp.zeros((self.ring, LANES), jnp.int32)
        table = jnp.zeros((self.ring, LANES), jnp.int32)
        held = CORES * self.passages
        for n in range(self.blocks * self.per_block):
            wanted = self.ids[n % self.per_block, n // self.per_block]
            owner = wanted // held
            here = (chip == owner) & (used < self.slots)
            table = jnp.where(here & (lane == used), n // self.per_block, table)
            table = jnp.where(here & (lane == self.slots + used), wanted - owner * held, table)
            table = jnp.where(lane == 2 * self.slots + n, jnp.where(here, used, self.slots), table)
            used = used + jnp.where(here, 1, 0)
        for i in range(self.ring):
            self.table[i] = table[i : i + 1]

    def entered(self):
        self.make_table()
        pl.semaphore_wait(pltpu.get_barrier_semaphore(), self.ring + self.n_tp - 1)
        for d in range(1, self.ring):
            self.send(self.table.at[lax.rem(self.y_me + d, self.ring)], self.tabv.at[self.ring - d], self.t_recv.at[0],
                      st=self.chip(d))
        self.own_table = pltpu.make_async_copy(self.table.at[self.y_me], self.tabv.at[0], self.s_sem.at[1])
        self.own_table.start()


    def part(self, rel, g):
        return self.qall[rel].at[pl.ds(self.per_group * g, self.per_group)]

    def queries(self, g):
        self.tok_loads[g].wait()
        if g == 0:
            self.first_loads[0].wait()
        normed_rows(self.xq, self.tok.at[pl.ds(g * 128, 128)], self.qgain, 128, unroll=4)
        if g == 0:
            self.first_loads[1].wait()
        q = jnp.dot(self.xq[...], self.wq[...], preferred_element_type=F32).astype(BF16)
        n = self.block_len
        for i in range(self.per_group):
            self.qall[0][self.per_group * g + i] = q[i * n : (i + 1) * n]
        if g == 0:
            with jax.named_scope("entry"):
                self.entered()
        for side, rel, who in ((0, self.ring - 1, self.right), (1, 1, self.left)):
            self.send(self.part(0, g), self.part(rel, g), self.q_recv.at[self.q_sem(side, 1, g)], st=who)

    def hand_on(self, side, hop, g, on):
        rel = self.ring - hop if side == 0 else hop
        here = self.part(rel, g)
        self.got(here, self.q_recv.at[self.q_sem(side, hop, g)])
        if on:
            there = self.part(rel - 1 if side == 0 else rel + 1, g)
            self.send(here, there, self.q_recv.at[self.q_sem(side, hop + 1, g)],
                      st=self.right if side == 0 else self.left)

    def q_sem(self, side, hop, g):
        last = (self.half - 1) * self.groups
        each = last + self.groups // 2
        return side * each + ((hop - 1) * self.groups + g if hop < self.half else last + g % (self.groups // 2))


    def norm_passages(self, p):
        for copy in self.kv_loads + self.store_loads[:2]:
            copy.wait()
        self.norm_half(p, 0, unroll=2)
        self.norm_half(p, 1, unroll=2)

    def norm_half(self, p, i, unroll=8):
        if p < self.passages:
            if p:
                self.store_loads[p + i].wait()
            normed_rows(self.xn.at[p // 2 % 2, pl.ds(i * 128, 128)], self.store.at[pl.ds((p + i) * 128, 128)], self.pgain,
                        128, unroll=unroll)

    def share(self, j, ref, p):
        both = ref.at[pl.ds(self.core * self.passages + p, 2)]
        self.send(both, both, self.kv_recv.at[j], st=self.partner)

    def keys(self, p):
        self.norm_half(p + 2, 0)
        k = jnp.dot(self.xn[p // 2 % 2], self.wk[...], preferred_element_type=F32).astype(BF16)
        for i in range(2):
            at = self.core * self.passages + p + i
            self.kall[at] = k[i * 128 : (i + 1) * 128]
        self.share(0, self.kall, p)

    def values(self, p):
        self.norm_half(p + 2, 1)
        v = jnp.dot(self.xn[p // 2 % 2], self.wv[...], preferred_element_type=F32)
        for i in range(2):
            at = self.core * self.passages + p + i
            w = v[i * 128 : (i + 1) * 128]
            self.vall[at] = jnp.concatenate([w[:, :LANES].T, w[:, LANES:].T], axis=1).astype(BF16)
        self.share(1, self.vall, p)

    def all_here(self):
        for j, ref in enumerate((self.kall, self.vall)):
            self.got(ref.at[pl.ds((1 - self.core) * self.passages, self.passages)], self.kv_recv.at[j])
        self.own_table.wait()
        self.got(self.tabv.at[pl.ds(1, self.ring - 1)], self.t_recv.at[0])
        to_scalar = pltpu.make_async_copy(self.tabv, self.tabs, self.s_sem.at[0])
        to_scalar.start()
        to_scalar.wait()


    def attend(self, rel):
        low_half = lax.broadcasted_iota(jnp.int32, (LANES, LANES), 1) < LANES // 2
        slots, tabs, ml, outs = self.slots, self.tabs, self.ml, self.outs
        for k in range(slots):
            q = self.qall[rel][tabs[rel, 0, k]]
            p = tabs[rel, 0, slots + k]
            s = lax.dot_general(
                self.kall[p], jnp.concatenate([q, q], axis=0), (((1,), (1,)), ((), ())), preferred_element_type=F32
            ) * HD ** (-0.5)
            top = jnp.max(s, axis=0, keepdims=True)
            e = jnp.exp(s - top)
            ml[k, 0:1] = top
            ml[k, 1:2] = jnp.sum(e, axis=0, keepdims=True)
            w = jnp.concatenate([jnp.where(low_half, e, 0.0), jnp.where(low_half, 0.0, e)], axis=0).astype(BF16)
            outs[k] = jnp.dot(self.vall[p], w, preferred_element_type=F32).astype(BF16)

    def join(self, rel):
        slots, tabs, ml, outs = self.slots, self.tabs, self.ml, self.outs

        @pl.loop(0, self.blocks, unroll=4)
        def _(distance):
            b = lax.rem(self.x_me + distance, self.blocks)
            at = [tabs[rel, 0, 2 * slots + b * self.per_block + j] for j in range(self.per_block)]
            mls = [ml[i] for i in at]
            best = functools.reduce(jnp.maximum, [a[0:1] for a in mls])
            scale = [jnp.exp(a[0:1] - best) for a in mls]
            total = sum(f * a[1:2] for f, a in zip(scale, mls))
            num = sum(f * outs[i].astype(F32) for f, i in zip(scale, at))
            place = place_of(distance, self.n_tp)
            self.acc[rel, place] = num.astype(BF16)
            self.stats[rel, place, 0:1] = best
            self.stats[rel, place, 1:2] = total


    def y_out(self, side, p, d, num, stat):
        who = self.right if side == 0 else self.left
        pairs = [(num, self.ydata.at[side, p, d - 1]), (stat, self.ystat.at[side, p, d - 1])]
        self.send_all(pairs, self.y_recv.at[self.y_sem(side, p, d - 1)], st=who)

    def y_sem(self, side, p, d):
        return sum(self.start_of(i, q) for q in range(1, p) for i in range(2)) + side * self.start_of(0, p) + d

    def y_start(self, side, p, d):
        rel = d if side == 0 else self.ring - d
        self.y_out(side, p, d, self.acc.at[rel, p], self.stats.at[rel, p])

    def y_arrived(self, side, p, d):
        self.got(self.both, self.y_recv.at[self.y_sem(side, p, d)])
        stat = self.ystat.at[side, p, d]
        return self.ydata[side, p, d].astype(F32), stat[0:1], stat[1:2]

    def own(self, rel, p):
        return self.acc[rel, p].astype(F32), self.stats[rel, p, 0:1], self.stats[rel, p, 1:2]

    def y_stage(self, side, p, d):
        so_far = merged(self.y_arrived(side, p, d), self.own(d if side == 0 else self.ring - d, p))
        if d == 1 and self.join_side(p) == side:
            so_far = merged(so_far, self.joined(p))
        num, best, total = so_far
        self.ydata[side, p, d] = num.astype(BF16)
        self.ystat[side, p, d, 0:1] = best
        self.ystat[side, p, d, 1:2] = total
        self.y_out(side, p, d, self.ydata.at[side, p, d], self.ystat.at[side, p, d])

    def join_side(self, p):
        early = [q for chunk in self.chunks[1 : self.early] for q in chunk]
        return early.index(p) % 2 if p in early else None

    def join_late(self, p):
        side = self.join_side(p)
        hops = self.half - 1
        who = self.chip(hops if side == 0 else self.ring - hops)
        pairs = [(self.acc.at[self.half, p], self.jdata.at[p]), (self.stats.at[self.half, p], self.jstat.at[p])]
        self.send_all(pairs, self.j_recv.at[p], st=who)

    def joined(self, p):
        self.got(self.both, self.j_recv.at[p])
        stat = self.jstat.at[p]
        return self.jdata[p].astype(F32), stat[0:1], stat[1:2]

    def direct(self, rel):
        p = self.chunks[0][0]
        at = self.ring - rel
        pairs = [(self.acc.at[rel, p], self.ddata.at[at]), (self.stats.at[rel, p], self.dstat.at[at])]
        self.send_all(pairs, self.d_recv.at[at - 1], st=self.chip(rel))

    def home(self, c):
        for i, p in enumerate(self.chunks[c]):
            if c == 0:
                so_far = self.own(0, p)
                for rel in range(1, self.ring):
                    self.got(self.both, self.d_recv.at[rel - 1])
                    stat = self.dstat.at[rel]
                    so_far = merged(so_far, (self.ddata[rel].astype(F32), stat[0:1], stat[1:2]))
            else:
                so_far = merged(merged(self.y_arrived(0, p, 0), self.own(0, p)), self.y_arrived(1, p, 0))
            num, best, total = so_far
            t = (num / total).T.astype(BF16)
            n = self.block_len
            self.rows_a[c, pl.ds(i * n, n), :] = jnp.concatenate([t[:n], t[n:]], axis=1)


    def glu(self, g):
        xm = self.xm
        if g == 0:
            for copy in self.glu_loads:
                copy.wait()
        normed_rows(xm, self.tok.at[pl.ds(g * 128, 128)], self.mgain, 128)
        y = jnp.dot(xm[...], self.wglu[...], preferred_element_type=F32)
        gated = y[:, :LANES] * jax.nn.sigmoid(y[:, LANES:])
        self.padded[g, pl.ds(16, 128), :] = gated.astype(BF16).astype(F32)

    def convolve(self, g):
        taps = self.taps[...].astype(F32)
        span = taps.shape[0]
        first = 16 - (span - 1) // 2
        running = jnp.zeros((128, LANES), F32)
        for k in range(span):
            running = running + self.padded[g, pl.ds(first + k, 128), :] * taps[k : k + 1]
        self.conv[g] = running
        turned = running.T
        self.sums[g : g + 1, :] = jnp.sum(turned, axis=0, keepdims=True)
        at = self.groups + g
        self.sums[at : at + 1, :] = jnp.sum(turned * turned, axis=0, keepdims=True)

    def send_sums(self):
        for d in range(1, self.n_tp):
            self.send(self.sums, self.allsums.at[self.n_tp - d], self.c_recv.at[0], tp=self.column(d))

    def activations(self):
        total = self.sums[...]
        self.got(self.allsums.at[pl.ds(1, self.n_tp - 1)], self.c_recv.at[0])
        for d in range(1, self.n_tp):
            total = total + self.allsums[d]
        groups = self.groups
        mean = total[:groups] / CA
        var = total[groups:] / CA - mean * mean
        cols = jnp.concatenate([mean, lax.rsqrt(var + EPS)], axis=0).T
        n = self.block_len
        for g in range(groups):
            z = (self.conv[g] - cols[:, g : g + 1]) * cols[:, groups + g : groups + g + 1] * self.cgain[...]
            z = (z / (1.0 + jnp.exp(-z))).astype(BF16)
            for i in range(self.per_group):
                self.act[g * self.per_group + i] = z[i * n : (i + 1) * n]


    def project(self, c, t, gets, outs):
        chunk, k, n = self.chunks[c], self.xhalf - c, self.block_len
        at = pl.ds(t * self.tile, self.tile)
        if c == 0 and t == 0:
            for copy in self.out_loads:
                copy.wait()
        rows_p = jnp.concatenate([self.act[self.column(self.places[p])] for p in chunk], axis=0)
        y = jnp.dot(rows_p, self.mix[:, at], preferred_element_type=F32) + self.blend[:, at] * jnp.dot(
            self.rows_a[c, pl.ds(0, n * len(chunk)), :], self.attn[:, at], preferred_element_type=F32
        )
        for side in gets:
            self.got(self.xdata.at[side, k, t], self.x_recv.at[self.x_sem(side, k, t)])
        if k == 0:
            y = y + self.xdata[0, k, t].astype(F32) + self.xdata[1, k, t].astype(F32)
            self.out[:, at] = y.astype(BF16)
            return
        for side in outs:
            mine = y if len(chunk) == 1 else y[side * n : (side + 1) * n]
            if side in gets:
                mine = mine + self.xdata[side, k, t].astype(F32)
            slot = self.xdata.at[side, k, t] if k < self.xhalf else self.xfirst.at[t]
            slot[...] = mine.astype(BF16)
            self.send(slot, self.xdata.at[side, k - 1, t], self.x_recv.at[self.x_sem(side, k - 1, t)],
                      tp=self.column(1 if side == 0 else self.n_tp - 1))

    def x_sem(self, side, k, t):
        return side * (self.xhalf - 1) * self.tiles + k * self.tiles + t if k < self.xhalf - 1 else (
            2 * (self.xhalf - 1) * self.tiles + t
        )


def whole_kernel(names, n_st, n_tp, slots, blocks, per_block, *refs):
    ring = n_st // CORES
    at = names.index("qall")
    found = dict(zip(names[:at] + names[at + 1 :], refs[:at] + refs[at + ring :]))
    found["qall"] = refs[at : at + ring]
    k = Body(n_st, n_tp, slots, blocks, per_block, found)
    plan = step_plan(k)
    with jax.named_scope("enter"):
        k.enter()
    for name, ready, end in plan.order(BACKLOG):
        gap = ready - k.clock
        while gap > 0.1 and k.waiting and k.waiting[0][0] < k.clock - 8.0:
            k.settle()
            gap -= 0.03
        with jax.named_scope("_".join(str(part) for part in name)):
            plan.steps[name][0]()
        k.clock = end
    with jax.named_scope(f"tail_{len(k.waiting)}"):
        while k.waiting:
            k.settle()


def whole(ids, slots, blocks, per_block, big, small):
    n_st, n_tp = lax.axis_size("st"), lax.axis_size("tp")
    ring, half, xhalf = n_st // CORES, n_st // CORES // 2, n_tp // 2
    rows, width = big["tok_hbm"].shape
    passages, prows, _ = big["store_hbm"].shape
    groups, block_len, mine = rows // 128, rows // blocks, rows // n_tp
    channels = big["gv_hbm"].shape[1]
    assert prows == 128 and big["wq_hbm"].shape[1] == HD and channels == LANES
    assert block_len * 2 == LANES and blocks == n_tp and passages % 2 == 0
    tiles = width // 512
    dma = pltpu.SemaphoreType.DMA
    scratch = {
        "tok": pltpu.VMEM((rows, width), BF16),
        "store": pltpu.VMEM((passages * prows, width), BF16),
        "wq": pltpu.VMEM((width, HD), BF16),
        "wk": pltpu.VMEM((width, HD), BF16),
        "wv": pltpu.VMEM((width, HD), BF16),
        "wglu": pltpu.VMEM((width, 2 * LANES), BF16),
        "attn": pltpu.VMEM((HD, width), BF16),
        "mix": pltpu.VMEM((channels, width), BF16),
        "xq": pltpu.VMEM((128, width), BF16),
        "xn": pltpu.VMEM((2, 256, width), BF16),
        "xm": pltpu.VMEM((128, width), BF16),
        "kall": pltpu.VMEM((CORES * passages, prows, HD), BF16),
        "vall": pltpu.VMEM((CORES * passages, LANES, 2 * prows), BF16),
        "outs": pltpu.VMEM((slots + 1, LANES, LANES), BF16),
        "ml": pltpu.VMEM((slots + 1, 2, LANES), F32),
        "tabv": pltpu.VMEM((ring, 1, LANES), jnp.int32),
        "tabs": pltpu.SMEM((ring, 1, LANES), jnp.int32),
        "acc": pltpu.VMEM((ring, blocks, LANES, LANES), BF16),
        "stats": pltpu.VMEM((ring, blocks, 2, LANES), F32),
        "ydata": pltpu.VMEM((2, blocks, half, LANES, LANES), BF16),
        "ystat": pltpu.VMEM((2, blocks, half, 2, LANES), F32),
        "ddata": pltpu.VMEM((ring, LANES, LANES), BF16),
        "dstat": pltpu.VMEM((ring, 2, LANES), F32),
        "both": pltpu.VMEM((1 + LANES * LANES * 2 // (2 * LANES * 4), 2, LANES), F32),
        "jdata": pltpu.VMEM((blocks, LANES, LANES), BF16),
        "jstat": pltpu.VMEM((blocks, 2, LANES), F32),
        "rows_a": pltpu.VMEM((xhalf + 1, 2 * block_len, HD), BF16),
        "padded": pltpu.VMEM((groups, 128 + 32, LANES), F32),
        "conv": pltpu.VMEM((groups, 128, LANES), F32),
        "sums": pltpu.VMEM((2 * groups, 128), F32),
        "allsums": pltpu.VMEM((n_tp, 2 * groups, 128), F32),
        "act": pltpu.VMEM((blocks, block_len, channels), BF16),
        "xdata": pltpu.VMEM((2, xhalf, tiles, mine, 512), BF16),
        "xfirst": pltpu.VMEM((tiles, mine, 512), BF16),
        "load_sem": dma((7 + groups + passages + len(small) + 1,)),
        "send_sem": dma((48,)),
        "q_recv": dma((2 * ((half - 1) * groups + groups // 2),)),
        "kv_recv": dma((2,)),
        "t_recv": dma((1,)),
        "s_sem": dma((2,)),
        "y_recv": dma(((blocks - 1) * (2 * half - 1),)),
        "d_recv": dma((ring - 1,)),
        "j_recv": dma((3,)),
        "x_recv": dma((2 * (xhalf - 1) * tiles + tiles,)),
        "c_recv": dma((1,)),
        "qall": None,
    }
    scratch = {**{n[:-4]: pltpu.VMEM(a.shape, a.dtype) for n, a in small.items()},
               "table": pltpu.VMEM((ring, 1, LANES), jnp.int32), "ids": pltpu.SMEM(ids.shape[::-1], jnp.int32), **scratch}
    names = list(big) + list(small) + ["ids_hbm", "out"] + list(scratch)
    shapes = [s for n, s in scratch.items() if n != "qall"]
    shapes += [pltpu.VMEM((blocks, block_len, HD), BF16) for _ in range(ring)]
    vmem = pl.BlockSpec(memory_space=pltpu.VMEM)
    return pl.pallas_call(
        functools.partial(whole_kernel, names, n_st, n_tp, slots, blocks, per_block),
        out_shape=jax.ShapeDtypeStruct((mine, width), BF16),
        in_specs=[pl.BlockSpec(memory_space=pltpu.HBM)] * (len(big) + len(small) + 1),
        out_specs=vmem,
        scratch_shapes=shapes,
        compiler_params=pltpu.CompilerParams(
            collective_id=0, has_side_effects=True, vmem_limit_bytes=66_000_000
        ),
        name="whole",
    )(*big.values(), *small.values(), ids.T)


def local(
    tokens, store, passage_ids, mix_gain, glu_value, glu_gate, conv_taps, channel_gain, mix_out,
    query_gain, passage_gain, query_proj, key_proj, value_proj, attn_out, blend_gain,
):
    owners = lax.axis_size("st")
    blocks, per_block = passage_ids.shape
    slots = CORES * (2 * blocks * per_block // owners)
    big = {
        "tok_hbm": tokens, "store_hbm": store, "wq_hbm": query_proj, "wk_hbm": key_proj, "wv_hbm": value_proj,
        "gv_hbm": glu_value, "gg_hbm": glu_gate, "attn_hbm": attn_out, "mix_hbm": mix_out,
    }
    small = {
        "qgain_hbm": query_gain[None], "pgain_hbm": passage_gain[None], "mgain_hbm": mix_gain[None], "taps_hbm": conv_taps,
        "cgain_hbm": channel_gain[None], "blend_hbm": blend_gain[None],
    }
    return whole(passage_ids, slots, blocks, per_block, big, small)


def solution(mesh):
    in_specs = (
        P(("grp", "st"), None),
        P(("grp", "st"), None, None),
        P(("grp", "st"), None),
        P(),
        P(None, "tp"),
        P(None, "tp"),
        P(None, "tp"),
        P("tp"),
        P("tp", None),
        P(),
        P(),
        P(None, "tp"),
        P(None, "tp"),
        P(None, "tp"),
        P("tp", None),
        P(),
    )
    out_specs = P(("grp", "st", "tp"), None)
    return jax.shard_map(local, mesh=mesh, in_specs=in_specs, out_specs=out_specs, check_vma=False)
```

```python
import functools

import jax
import jax.numpy as jnp
from jax import lax
from jax.experimental import pallas as pl
from jax.experimental.pallas import tpu as pltpu
from jax.sharding import PartitionSpec as P

CA = 1024
HD = 256
SEQ_LEN = 128
CORES = 2
LANES = 128
EPS = 1e-06
EMPTY = -1e30
BACKLOG = {6: 1.5, 7: 1.5, 8: 0.8, 9: 0.3}
GATE = {3: 3, 4: 3}
MESH = pl.DeviceIdType.MESH
F32 = jnp.float32
BF16 = jnp.bfloat16


def remote(src, dst, send_sem, recv_sem, **target):
    return pltpu.make_async_remote_copy(
        src_ref=src, dst_ref=dst, send_sem=send_sem, recv_sem=recv_sem,
        device_id=target, device_id_type=MESH,
    )


def place_of(distance, n):
    half = n // 2
    return jnp.where(distance >= half, 2 * (distance - half), 2 * (half - distance) - 1)


def order_of(n):
    half = n // 2
    order = [half]
    for j in range(1, half):
        order += [half - j, half + j]
    return order + [0]


def normed_rows(dst, src, gain, rows, step=16, unroll=2):
    @pl.loop(0, rows // step, unroll=unroll)
    def _(i):
        at = pl.ds(pl.multiple_of(i * step, step), step)
        x = src[at, :].astype(F32)
        inv = lax.rsqrt(jnp.mean(x * x, axis=-1, keepdims=True) + EPS)
        dst[at, :] = (x * inv * gain[...]).astype(BF16)


def merged(a, b):
    best = jnp.maximum(a[1], b[1])
    fa, fb = jnp.exp(a[1] - best), jnp.exp(b[1] - best)
    return fa * a[0] + fb * b[0], best, fa * a[2] + fb * b[2]


class Plan:
    def __init__(self):
        self.steps = {}

    def add(self, name, run, time, rank, after=(), gets=(), sends=()):
        self.steps[name] = (run, time, rank, tuple(after), tuple(gets), tuple(sends))

    def order(self, backlog):
        clock, free, arrival, done, order = 0.0, {}, {}, set(), []
        left = list(self.steps)
        while left:
            best = None
            for name in left:
                _, _, rank, after, gets, sends = self.steps[name]
                if all(a in done for a in after) and all(g in arrival for g in gets):
                    ready = max([clock] + [arrival[g] for g in gets])
                    if rank in backlog:
                        ready = max([ready] + [free.get(link, 0.0) - backlog[rank] for _, link, *_ in sends])
                    if best is None or (ready, rank) < best[0]:
                        best = ((ready, rank), name)
            (ready, _), name = best
            _, time, _, _, _, sends = self.steps[name]
            clock = ready + time
            for message, link, wire, late, *hops in sends:
                free[link] = max(free.get(link, 0.0), clock) + wire
                arrival[message] = free[link] + late
                free[link] += wire * (hops[0] - 1 if hops else 0)
            done.add(name)
            left.remove(name)
            order.append((name, ready, clock))
        return order


def step_plan(k):
    plan = Plan()
    ring, half, groups, xhalf = k.ring, k.half, k.groups, k.xhalf
    hop_late, far_late, q_wire, y_wire, x_wire = 2.6, 0.75, 1.4, 0.72, 1.4
    for g in range(groups):
        plan.add(
            ("q", g), functools.partial(k.queries, g), 0.76, 1, [("q", g - 1)] if g else [],
            sends=[(("q", side, 1, h), ("y", side), q_wire, hop_late) for side, h in k.first_sends(g)],
        )
    for hop in range(1, half + 1):
        for g in range(groups):
            for side in range(2):
                if hop == half and (g < groups // 2) != (side == 0):
                    continue
                on = hop + 1 < half or (hop + 1 == half and (g < groups // 2) == (side == 0))
                plan.add(
                    ("hand", side, hop, g), functools.partial(k.hand_on, side, hop, g, on), 0.03, 0,
                    gets=[("q", side, hop, g)],
                    sends=[(("q", side, hop + 1, g), ("y", side), q_wire, hop_late)] if on else [],
                )
    pairs = list(range(0, k.passages, 2))
    for p in pairs:
        if p == 0:
            plan.add(("norm", p), functools.partial(k.norm_passages, p), 1.0, 20, [("q", groups - 1)])
        plan.add(("k", p), functools.partial(k.keys, p), 0.77, 20, [("v", p - 2) if p else ("norm", p)])
        plan.add(("v", p), functools.partial(k.values, p), 0.86, 20, [("k", p)], sends=[(("kv", p), ("core",), 0.4, 1.0)])
    plan.add(("here",), k.all_here, 0.65, 21, [("v", p) for p in pairs], gets=[("kv", p) for p in pairs])
    for rel in range(ring):
        hop = min(rel, ring - rel)
        if hop == half:
            hands = [("hand", 0 if g < groups // 2 else 1, hop, g) for g in range(groups)]
        elif hop:
            hands = [("hand", 1 if rel < half else 0, hop, g) for g in range(groups)]
        else:
            hands = []
        plan.add(("slots", rel), functools.partial(k.attend, rel), 0.62, 19 - hop, [("here",)] + hands)
        plan.add(("attend", rel), functools.partial(k.join, rel), 0.3, 1, [("slots", rel)])
    last_hands = [("hand", 0 if g < groups // 2 else 1, half - 1, g) for g in range(groups)]
    for rel in range(1, ring):
        hop = min(rel, ring - rel)
        plan.add(
            ("direct", rel), functools.partial(k.direct, rel), 0.04, 2, [("attend", rel)] + last_hands,
            sends=[(("direct", ring - rel), ("y", 0 if rel <= half else 1), y_wire, hop_late + far_late * (hop - 1), hop)],
        )
    for c, chunk in enumerate(k.chunks[1:], 1):
        for p in chunk:
            joined = k.join_side(p)
            if joined is not None:
                plan.add(
                    ("join", p), functools.partial(k.join_late, p), 0.04, 5 + c, [("attend", half)],
                    sends=[(("join", p), ("y", joined), y_wire, hop_late + far_late * (half - 2), half - 1)],
                )
            for side in range(2):
                far = k.start_of(side, p)
                gate = GATE.get(c, 0)
                gated = [("y", side, q, gate) for q in k.chunks[c - 1]] if gate else []
                for d in range(far, 0, -1):
                    rel = d if side == 0 else ring - d
                    gets = [] if d == far else [("y", side, p, d)]
                    if joined == side and d == 1:
                        gets = gets + [("join", p)]
                    plan.add(
                        ("y", side, p, d),
                        functools.partial(k.y_start if d == far else k.y_stage, side, p, d), 0.04 if d == far else 0.06,
                        5 + c, [("attend", rel)] + (gated if d == far else []), gets=gets,
                        sends=[(("y", side, p, d - 1), ("y", side), y_wire, hop_late)],
                    )
    for g in range(groups):
        plan.add(("glu", g), functools.partial(k.glu, g), 0.95, 30, [("q", groups - 1)])
        plan.add(("conv", g), functools.partial(k.convolve, g), 0.25, 29, [("glu", g)])
    plan.add(("sums",), k.send_sums, 0.1, 3, [("conv", g) for g in range(groups)],
             sends=[(("sums",), ("x", 2), 0.5, 5.0)])
    plan.add(("act",), k.activations, 0.4, 4, gets=[("sums",)])
    for c, chunk in enumerate(k.chunks):
        if c == 0:
            gets = [("direct", rel) for rel in range(1, ring)]
        else:
            gets = [("y", side, p, 0) for p in chunk for side in range(2)]
        plan.add(("home", c), functools.partial(k.home, c), 0.3, 4, [("attend", 0)], gets=gets)
        dist = xhalf - c
        for t in range(k.tiles):
            h = t // (k.tiles // 2)
            if dist == xhalf:
                gets, outs = [], [h]
            elif dist == 0:
                gets, outs = [0, 1], []
            else:
                gets = [0, 1] if dist < xhalf - 1 else [h]
                outs = [0, 1]
            plan.add(
                ("project", c, t), functools.partial(k.project, c, t, gets, outs), 0.25, 3, [("home", c), ("act",)],
                gets=[("x", side, dist, t) for side in gets],
                sends=[(("x", side, dist - 1, t), ("x", side), x_wire, hop_late) for side in outs],
            )
    return plan


class Body:
    def __init__(self, n_st, n_tp, slots, blocks, per_block, refs):
        self.__dict__.update(refs)
        self.n_st, self.n_tp, self.slots, self.blocks, self.per_block = n_st, n_tp, slots, blocks, per_block
        self.ring, self.groups = n_st // CORES, self.tok_hbm.shape[0] // 128
        self.half, self.xhalf = self.ring // 2, n_tp // 2
        self.passages = self.store_hbm.shape[0]
        self.per_group = blocks // self.groups
        self.block_len = 128 // self.per_group
        self.width = self.tok_hbm.shape[1]
        self.tile = 512
        self.tiles = self.width // self.tile
        self.me, self.x_me = lax.axis_index("st"), lax.axis_index("tp")
        self.core, self.y_me = lax.rem(self.me, CORES), self.me // CORES
        self.partner = self.me + 1 - 2 * self.core
        self.right, self.left = self.chip(1), self.chip(self.ring - 1)
        self.results = []
        self.waiting, self.unused, self.loads, self.clock = [], list(range(refs["send_sem"].shape[0])), [], 0.0
        self.early = 2
        self.places = order_of(n_tp)
        self.chunks = [[0]] + [[2 * j - 1, 2 * j] for j in range(1, self.xhalf)] + [[n_tp - 1]]
        self.start_cw = {}
        for c, chunk in enumerate(self.chunks):
            for i, p in enumerate(chunk):
                self.start_cw[p] = self.half if (i == 0 and c < len(self.chunks) - 1) else self.half - 1

    def chip(self, d):
        return lax.rem(self.me + CORES * d, self.n_st)

    def column(self, d):
        return lax.rem(self.x_me + d, self.n_tp)

    def send(self, src, dst, recv_sem, **target):
        self.send_all([(src, dst)], recv_sem, **target)

    def send_all(self, pairs, recv_sem, **target):
        if not self.unused:
            self.settle()
        at = self.unused.pop(0)
        sem = self.send_sem.at[at]
        for src, dst in pairs:
            remote(src, dst, sem, recv_sem, **target).start()
        whole = self.both if len(pairs) > 1 else pairs[0][0]
        self.waiting.append((self.clock, remote(whole, whole, sem, recv_sem, **target), at))

    def settle(self):
        _, copy, at = self.waiting.pop(0)
        copy.wait_send()
        self.unused.append(at)

    def got(self, ref, recv_sem):
        remote(ref, ref, self.send_sem.at[0], recv_sem, st=self.partner).wait_recv()

    def load(self, src, dst):
        copy = pltpu.make_async_copy(src, dst, self.load_sem.at[len(self.loads)])
        copy.start()
        self.loads.append(copy)
        return copy

    def start_of(self, side, p):
        if self.join_side(p) is not None:
            return self.half - 1
        return self.start_cw[p] if side == 0 else 2 * self.half - 1 - self.start_cw[p]

    def enter(self):
        small = lambda name: self.load(getattr(self, name + "_hbm"), getattr(self, name))
        self.first_loads = [small("qgain"), self.load(self.wq_hbm, self.wq)]
        rows = lambda g: pl.ds(g * 128, 128)
        self.tok_loads = [self.load(self.tok_hbm.at[rows(g)], self.tok.at[rows(g)]) for g in range(self.groups)]
        self.ids_load = small("ids")
        self.kv_loads = [small("pgain"), self.load(self.wk_hbm, self.wk), self.load(self.wv_hbm, self.wv)]
        self.store_loads = [
            self.load(self.store_hbm.at[p], self.store.at[pl.ds(p * 128, 128)]) for p in range(self.passages)
        ]
        self.glu_loads = [
            small("mgain"), small("taps"), small("cgain"),
            self.load(self.gv_hbm, self.wglu.at[:, pl.ds(0, LANES)]),
            self.load(self.gg_hbm, self.wglu.at[:, pl.ds(LANES, LANES)]),
        ]
        self.out_loads = [small("blend"), self.load(self.attn_hbm, self.attn), self.load(self.mix_hbm, self.mix)]
        barrier = pltpu.get_barrier_semaphore()
        for d in range(1, self.ring):
            pl.semaphore_signal(barrier, inc=1, device_id={"st": self.chip(d)}, device_id_type=MESH)
        pl.semaphore_signal(barrier, inc=1, device_id={"st": self.partner}, device_id_type=MESH)
        for d in range(1, self.n_tp):
            pl.semaphore_signal(barrier, inc=1, device_id={"tp": self.column(d)}, device_id_type=MESH)
        s = self.slots
        self.outs[s] = jnp.zeros(self.outs.shape[1:], BF16)
        self.ml[s, 0:1] = jnp.full((1, LANES), EMPTY, F32)
        self.ml[s, 1:2] = jnp.zeros((1, LANES), F32)
        self.padded[...] = jnp.zeros(self.padded.shape, F32)

    def make_table(self):
        self.ids_load.wait()
        chip = lax.broadcasted_iota(jnp.int32, (self.ring, LANES), 0)
        lane = lax.broadcasted_iota(jnp.int32, (self.ring, LANES), 1)
        used = jnp.zeros((self.ring, LANES), jnp.int32)
        table = jnp.zeros((self.ring, LANES), jnp.int32)
        held = CORES * self.passages
        for n in range(self.blocks * self.per_block):
            wanted = self.ids[n % self.per_block, n // self.per_block]
            owner = wanted // held
            here = (chip == owner) & (used < self.slots)
            table = jnp.where(here & (lane == used), n // self.per_block, table)
            table = jnp.where(here & (lane == self.slots + used), wanted - owner * held, table)
            table = jnp.where(lane == 2 * self.slots + n, jnp.where(here, used, self.slots), table)
            used = used + jnp.where(here, 1, 0)
        for i in range(self.ring):
            self.table[i] = table[i : i + 1]

    def entered(self):
        self.make_table()
        pl.semaphore_wait(pltpu.get_barrier_semaphore(), self.ring + self.n_tp - 1)
        for d in range(1, self.ring):
            self.send(self.table.at[lax.rem(self.y_me + d, self.ring)], self.tabv.at[self.ring - d], self.t_recv.at[0],
                      st=self.chip(d))
        self.own_table = pltpu.make_async_copy(self.table.at[self.y_me], self.tabv.at[0], self.s_sem.at[1])
        self.own_table.start()


    def part(self, rel, g):
        return self.qall[rel].at[pl.ds(self.per_group * g, self.per_group)]

    def queries(self, g):
        self.tok_loads[g].wait()
        if g == 0:
            self.first_loads[0].wait()
        normed_rows(self.xq, self.tok.at[pl.ds(g * 128, 128)], self.qgain, 128, unroll=4)
        if g == 0:
            self.first_loads[1].wait()
        q = jnp.dot(self.xq[...], self.wq[...], preferred_element_type=F32).astype(BF16)
        n = self.block_len
        for i in range(self.per_group):
            self.qall[0][self.per_group * g + i] = q[i * n : (i + 1) * n]
        if g == 0:
            with jax.named_scope("entry"):
                self.entered()
        for side, h in self.first_sends(g):
            rel, who = ((self.ring - 1, self.right), (1, self.left))[side]
            self.send(self.part(0, h), self.part(rel, h), self.q_recv.at[self.q_sem(side, 1, h)], st=who)

    def first_sends(self, g):
        n = self.groups
        if g == 0:
            left = [0]
        else:
            left = [g] if g >= n // 2 else []
        return [(0, g)] + [(1, h) for h in left] + ([(1, h) for h in range(1, n // 2)] if g == n - 1 else [])

    def hand_on(self, side, hop, g, on):
        rel = self.ring - hop if side == 0 else hop
        here = self.part(rel, g)
        self.got(here, self.q_recv.at[self.q_sem(side, hop, g)])
        if on:
            there = self.part(rel - 1 if side == 0 else rel + 1, g)
            self.send(here, there, self.q_recv.at[self.q_sem(side, hop + 1, g)],
                      st=self.right if side == 0 else self.left)

    def q_sem(self, side, hop, g):
        last = (self.half - 1) * self.groups
        each = last + self.groups // 2
        return side * each + ((hop - 1) * self.groups + g if hop < self.half else last + g % (self.groups // 2))


    def norm_passages(self, p):
        for copy in self.kv_loads + self.store_loads[:2]:
            copy.wait()
        self.norm_half(p, 0, unroll=2)
        self.norm_half(p, 1, unroll=2)

    def norm_half(self, p, i, unroll=8):
        if p < self.passages:
            if p:
                self.store_loads[p + i].wait()
            normed_rows(self.xn.at[p // 2 % 2, pl.ds(i * 128, 128)], self.store.at[pl.ds((p + i) * 128, 128)], self.pgain,
                        128, unroll=unroll)

    def share(self, j, ref, p):
        both = ref.at[pl.ds(self.core * self.passages + p, 2)]
        self.send(both, both, self.kv_recv.at[j], st=self.partner)

    def keys(self, p):
        self.norm_half(p + 2, 0)
        k = jnp.dot(self.xn[p // 2 % 2], self.wk[...], preferred_element_type=F32).astype(BF16)
        for i in range(2):
            at = self.core * self.passages + p + i
            self.kall[at] = k[i * 128 : (i + 1) * 128]
        self.share(0, self.kall, p)

    def values(self, p):
        self.norm_half(p + 2, 1)
        v = jnp.dot(self.xn[p // 2 % 2], self.wv[...], preferred_element_type=F32)
        for i in range(2):
            at = self.core * self.passages + p + i
            w = v[i * 128 : (i + 1) * 128]
            self.vall[at] = jnp.concatenate([w[:, :LANES].T, w[:, LANES:].T], axis=1).astype(BF16)
        self.share(1, self.vall, p)

    def all_here(self):
        for j, ref in enumerate((self.kall, self.vall)):
            self.got(ref.at[pl.ds((1 - self.core) * self.passages, self.passages)], self.kv_recv.at[j])
        self.own_table.wait()
        self.got(self.tabv.at[pl.ds(1, self.ring - 1)], self.t_recv.at[0])
        to_scalar = pltpu.make_async_copy(self.tabv, self.tabs, self.s_sem.at[0])
        to_scalar.start()
        to_scalar.wait()


    def attend(self, rel):
        low_half = lax.broadcasted_iota(jnp.int32, (LANES, LANES), 1) < LANES // 2
        slots, tabs, ml, outs = self.slots, self.tabs, self.ml, self.outs
        for k in range(slots):
            q = self.qall[rel][tabs[rel, 0, k]]
            p = tabs[rel, 0, slots + k]
            s = lax.dot_general(
                self.kall[p], jnp.concatenate([q, q], axis=0), (((1,), (1,)), ((), ())), preferred_element_type=F32
            ) * HD ** (-0.5)
            top = jnp.max(s, axis=0, keepdims=True)
            e = jnp.exp(s - top)
            ml[k, 0:1] = top
            ml[k, 1:2] = jnp.sum(e, axis=0, keepdims=True)
            w = jnp.concatenate([jnp.where(low_half, e, 0.0), jnp.where(low_half, 0.0, e)], axis=0).astype(BF16)
            outs[k] = jnp.dot(self.vall[p], w, preferred_element_type=F32).astype(BF16)

    def join(self, rel):
        slots, tabs, ml, outs = self.slots, self.tabs, self.ml, self.outs

        @pl.loop(0, self.blocks, unroll=4)
        def _(distance):
            b = lax.rem(self.x_me + distance, self.blocks)
            at = [tabs[rel, 0, 2 * slots + b * self.per_block + j] for j in range(self.per_block)]
            mls = [ml[i] for i in at]
            best = functools.reduce(jnp.maximum, [a[0:1] for a in mls])
            scale = [jnp.exp(a[0:1] - best) for a in mls]
            total = sum(f * a[1:2] for f, a in zip(scale, mls))
            num = sum(f * outs[i].astype(F32) for f, i in zip(scale, at))
            place = place_of(distance, self.n_tp)
            self.acc[rel, place] = num.astype(BF16)
            self.stats[rel, place, 0:1] = best
            self.stats[rel, place, 1:2] = total


    def y_out(self, side, p, d, num, stat):
        who = self.right if side == 0 else self.left
        pairs = [(num, self.ydata.at[side, p, d - 1]), (stat, self.ystat.at[side, p, d - 1])]
        self.send_all(pairs, self.y_recv.at[self.y_sem(side, p, d - 1)], st=who)

    def y_sem(self, side, p, d):
        return sum(self.start_of(i, q) for q in range(1, p) for i in range(2)) + side * self.start_of(0, p) + d

    def y_start(self, side, p, d):
        rel = d if side == 0 else self.ring - d
        self.y_out(side, p, d, self.acc.at[rel, p], self.stats.at[rel, p])

    def y_arrived(self, side, p, d):
        self.got(self.both, self.y_recv.at[self.y_sem(side, p, d)])
        stat = self.ystat.at[side, p, d]
        return self.ydata[side, p, d].astype(F32), stat[0:1], stat[1:2]

    def own(self, rel, p):
        return self.acc[rel, p].astype(F32), self.stats[rel, p, 0:1], self.stats[rel, p, 1:2]

    def y_stage(self, side, p, d):
        so_far = merged(self.y_arrived(side, p, d), self.own(d if side == 0 else self.ring - d, p))
        if d == 1 and self.join_side(p) == side:
            so_far = merged(so_far, self.joined(p))
        num, best, total = so_far
        self.ydata[side, p, d] = num.astype(BF16)
        self.ystat[side, p, d, 0:1] = best
        self.ystat[side, p, d, 1:2] = total
        self.y_out(side, p, d, self.ydata.at[side, p, d], self.ystat.at[side, p, d])

    def join_side(self, p):
        early = [q for chunk in self.chunks[1 : self.early] for q in chunk]
        return early.index(p) % 2 if p in early else None

    def join_late(self, p):
        side = self.join_side(p)
        hops = self.half - 1
        who = self.chip(hops if side == 0 else self.ring - hops)
        pairs = [(self.acc.at[self.half, p], self.jdata.at[p]), (self.stats.at[self.half, p], self.jstat.at[p])]
        self.send_all(pairs, self.j_recv.at[p], st=who)

    def joined(self, p):
        self.got(self.both, self.j_recv.at[p])
        stat = self.jstat.at[p]
        return self.jdata[p].astype(F32), stat[0:1], stat[1:2]

    def direct(self, rel):
        p = self.chunks[0][0]
        at = self.ring - rel
        pairs = [(self.acc.at[rel, p], self.ddata.at[at]), (self.stats.at[rel, p], self.dstat.at[at])]
        self.send_all(pairs, self.d_recv.at[at - 1], st=self.chip(rel))

    def home(self, c):
        for i, p in enumerate(self.chunks[c]):
            if c == 0:
                so_far = self.own(0, p)
                for rel in range(1, self.ring):
                    self.got(self.both, self.d_recv.at[rel - 1])
                    stat = self.dstat.at[rel]
                    so_far = merged(so_far, (self.ddata[rel].astype(F32), stat[0:1], stat[1:2]))
            else:
                so_far = merged(merged(self.y_arrived(0, p, 0), self.own(0, p)), self.y_arrived(1, p, 0))
            num, best, total = so_far
            t = (num / total).T.astype(BF16)
            n = self.block_len
            self.rows_a[c, pl.ds(i * n, n), :] = jnp.concatenate([t[:n], t[n:]], axis=1)


    def glu(self, g):
        xm = self.xm
        if g == 0:
            for copy in self.glu_loads:
                copy.wait()
        normed_rows(xm, self.tok.at[pl.ds(g * 128, 128)], self.mgain, 128)
        y = jnp.dot(xm[...], self.wglu[...], preferred_element_type=F32)
        gated = y[:, :LANES] * jax.nn.sigmoid(y[:, LANES:])
        self.padded[g, pl.ds(16, 128), :] = gated.astype(BF16).astype(F32)

    def convolve(self, g):
        taps = self.taps[...].astype(F32)
        span = taps.shape[0]
        first = 16 - (span - 1) // 2
        running = jnp.zeros((128, LANES), F32)
        for k in range(span):
            running = running + self.padded[g, pl.ds(first + k, 128), :] * taps[k : k + 1]
        self.conv[g] = running
        turned = running.T
        self.sums[g : g + 1, :] = jnp.sum(turned, axis=0, keepdims=True)
        at = self.groups + g
        self.sums[at : at + 1, :] = jnp.sum(turned * turned, axis=0, keepdims=True)

    def send_sums(self):
        for d in range(1, self.n_tp):
            self.send(self.sums, self.allsums.at[self.n_tp - d], self.c_recv.at[0], tp=self.column(d))

    def activations(self):
        total = self.sums[...]
        self.got(self.allsums.at[pl.ds(1, self.n_tp - 1)], self.c_recv.at[0])
        for d in range(1, self.n_tp):
            total = total + self.allsums[d]
        groups = self.groups
        mean = total[:groups] / CA
        var = total[groups:] / CA - mean * mean
        cols = jnp.concatenate([mean, lax.rsqrt(var + EPS)], axis=0).T
        n = self.block_len
        for g in range(groups):
            z = (self.conv[g] - cols[:, g : g + 1]) * cols[:, groups + g : groups + g + 1] * self.cgain[...]
            z = (z / (1.0 + jnp.exp(-z))).astype(BF16)
            for i in range(self.per_group):
                self.act[g * self.per_group + i] = z[i * n : (i + 1) * n]


    def project(self, c, t, gets, outs):
        chunk, k, n = self.chunks[c], self.xhalf - c, self.block_len
        at = pl.ds(t * self.tile, self.tile)
        if c == 0 and t == 0:
            for copy in self.out_loads:
                copy.wait()
        rows_p = jnp.concatenate([self.act[self.column(self.places[p])] for p in chunk], axis=0)
        y = jnp.dot(rows_p, self.mix[:, at], preferred_element_type=F32) + self.blend[:, at] * jnp.dot(
            self.rows_a[c, pl.ds(0, n * len(chunk)), :], self.attn[:, at], preferred_element_type=F32
        )
        for side in gets:
            self.got(self.xdata.at[side, k, t], self.x_recv.at[self.x_sem(side, k, t)])
        if k == 0:
            y = y + self.xdata[0, k, t].astype(F32) + self.xdata[1, k, t].astype(F32)
            self.tile_out[t] = y.astype(BF16)
            copy = pltpu.make_async_copy(self.tile_out.at[t], self.out.at[:, at], self.out_sem.at[t])
            copy.start()
            self.results.append(copy)
            return
        for side in outs:
            mine = y if len(chunk) == 1 else y[side * n : (side + 1) * n]
            if side in gets:
                mine = mine + self.xdata[side, k, t].astype(F32)
            slot = self.xdata.at[side, k, t] if k < self.xhalf else self.xfirst.at[t]
            slot[...] = mine.astype(BF16)
            self.send(slot, self.xdata.at[side, k - 1, t], self.x_recv.at[self.x_sem(side, k - 1, t)],
                      tp=self.column(1 if side == 0 else self.n_tp - 1))

    def x_sem(self, side, k, t):
        return side * (self.xhalf - 1) * self.tiles + k * self.tiles + t if k < self.xhalf - 1 else (
            2 * (self.xhalf - 1) * self.tiles + t
        )


def whole_kernel(names, n_st, n_tp, slots, blocks, per_block, *refs):
    ring = n_st // CORES
    at = names.index("qall")
    found = dict(zip(names[:at] + names[at + 1 :], refs[:at] + refs[at + ring :]))
    found["qall"] = refs[at : at + ring]
    k = Body(n_st, n_tp, slots, blocks, per_block, found)
    plan = step_plan(k)
    with jax.named_scope("enter"):
        k.enter()
    for name, ready, end in plan.order(BACKLOG):
        gap = ready - k.clock
        while gap > 0.1 and k.waiting and k.waiting[0][0] < k.clock - 8.0:
            k.settle()
            gap -= 0.03
        with jax.named_scope("_".join(str(part) for part in name)):
            plan.steps[name][0]()
        k.clock = end
    with jax.named_scope(f"tail_{len(k.waiting)}"):
        while k.waiting:
            k.settle()
        for copy in k.results:
            copy.wait()


def whole(ids, slots, blocks, per_block, big, small):
    n_st, n_tp = lax.axis_size("st"), lax.axis_size("tp")
    ring, half, xhalf = n_st // CORES, n_st // CORES // 2, n_tp // 2
    rows, width = big["tok_hbm"].shape
    passages, prows, _ = big["store_hbm"].shape
    groups, block_len, mine = rows // 128, rows // blocks, rows // n_tp
    channels = big["gv_hbm"].shape[1]
    assert prows == 128 and big["wq_hbm"].shape[1] == HD and channels == LANES
    assert block_len * 2 == LANES and blocks == n_tp and passages % 2 == 0
    tiles = width // 512
    dma = pltpu.SemaphoreType.DMA
    scratch = {
        "tok": pltpu.VMEM((rows, width), BF16),
        "store": pltpu.VMEM((passages * prows, width), BF16),
        "wq": pltpu.VMEM((width, HD), BF16),
        "wk": pltpu.VMEM((width, HD), BF16),
        "wv": pltpu.VMEM((width, HD), BF16),
        "wglu": pltpu.VMEM((width, 2 * LANES), BF16),
        "attn": pltpu.VMEM((HD, width), BF16),
        "mix": pltpu.VMEM((channels, width), BF16),
        "xq": pltpu.VMEM((128, width), BF16),
        "xn": pltpu.VMEM((2, 256, width), BF16),
        "xm": pltpu.VMEM((128, width), BF16),
        "kall": pltpu.VMEM((CORES * passages, prows, HD), BF16),
        "vall": pltpu.VMEM((CORES * passages, LANES, 2 * prows), BF16),
        "outs": pltpu.VMEM((slots + 1, LANES, LANES), BF16),
        "ml": pltpu.VMEM((slots + 1, 2, LANES), F32),
        "tabv": pltpu.VMEM((ring, 1, LANES), jnp.int32),
        "tabs": pltpu.SMEM((ring, 1, LANES), jnp.int32),
        "acc": pltpu.VMEM((ring, blocks, LANES, LANES), BF16),
        "stats": pltpu.VMEM((ring, blocks, 2, LANES), F32),
        "ydata": pltpu.VMEM((2, blocks, half, LANES, LANES), BF16),
        "ystat": pltpu.VMEM((2, blocks, half, 2, LANES), F32),
        "ddata": pltpu.VMEM((ring, LANES, LANES), BF16),
        "dstat": pltpu.VMEM((ring, 2, LANES), F32),
        "both": pltpu.VMEM((1 + LANES * LANES * 2 // (2 * LANES * 4), 2, LANES), F32),
        "jdata": pltpu.VMEM((blocks, LANES, LANES), BF16),
        "jstat": pltpu.VMEM((blocks, 2, LANES), F32),
        "rows_a": pltpu.VMEM((xhalf + 1, 2 * block_len, HD), BF16),
        "padded": pltpu.VMEM((groups, 128 + 32, LANES), F32),
        "conv": pltpu.VMEM((groups, 128, LANES), F32),
        "sums": pltpu.VMEM((2 * groups, 128), F32),
        "allsums": pltpu.VMEM((n_tp, 2 * groups, 128), F32),
        "act": pltpu.VMEM((blocks, block_len, channels), BF16),
        "xdata": pltpu.VMEM((2, xhalf, tiles, mine, 512), BF16),
        "xfirst": pltpu.VMEM((tiles, mine, 512), BF16),
        "load_sem": dma((7 + groups + passages + len(small) + 1,)),
        "tile_out": pltpu.VMEM((tiles, mine, 512), BF16),
        "out_sem": dma((tiles,)),
        "send_sem": dma((40,)),
        "q_recv": dma((2 * ((half - 1) * groups + groups // 2),)),
        "kv_recv": dma((2,)),
        "t_recv": dma((1,)),
        "s_sem": dma((2,)),
        "y_recv": dma(((blocks - 1) * (2 * half - 1),)),
        "d_recv": dma((ring - 1,)),
        "j_recv": dma((3,)),
        "x_recv": dma((2 * (xhalf - 1) * tiles + tiles,)),
        "c_recv": dma((1,)),
        "qall": None,
    }
    scratch = {**{n[:-4]: pltpu.VMEM(a.shape, a.dtype) for n, a in small.items()},
               "table": pltpu.VMEM((ring, 1, LANES), jnp.int32), "ids": pltpu.SMEM(ids.shape[::-1], jnp.int32), **scratch}
    names = list(big) + list(small) + ["ids_hbm", "out"] + list(scratch)
    shapes = [s for n, s in scratch.items() if n != "qall"]
    shapes += [pltpu.VMEM((blocks, block_len, HD), BF16) for _ in range(ring)]
    return pl.pallas_call(
        functools.partial(whole_kernel, names, n_st, n_tp, slots, blocks, per_block),
        out_shape=jax.ShapeDtypeStruct((mine, width), BF16),
        in_specs=[pl.BlockSpec(memory_space=pltpu.HBM)] * (len(big) + len(small) + 1),
        out_specs=pl.BlockSpec(memory_space=pltpu.HBM),
        scratch_shapes=shapes,
        compiler_params=pltpu.CompilerParams(
            collective_id=0, has_side_effects=True, vmem_limit_bytes=66_000_000
        ),
        name="whole",
    )(*big.values(), *small.values(), ids.T)


def local(
    tokens, store, passage_ids, mix_gain, glu_value, glu_gate, conv_taps, channel_gain, mix_out,
    query_gain, passage_gain, query_proj, key_proj, value_proj, attn_out, blend_gain,
):
    owners = lax.axis_size("st")
    blocks, per_block = passage_ids.shape
    slots = CORES * (2 * blocks * per_block // owners)
    big = {
        "tok_hbm": tokens, "store_hbm": store, "wq_hbm": query_proj, "wk_hbm": key_proj, "wv_hbm": value_proj,
        "gv_hbm": glu_value, "gg_hbm": glu_gate, "attn_hbm": attn_out, "mix_hbm": mix_out,
    }
    small = {
        "qgain_hbm": query_gain[None], "pgain_hbm": passage_gain[None], "mgain_hbm": mix_gain[None], "taps_hbm": conv_taps,
        "cgain_hbm": channel_gain[None], "blend_hbm": blend_gain[None],
    }
    return whole(passage_ids, slots, blocks, per_block, big, small)


def solution(mesh):
    in_specs = (
        P(("grp", "st"), None),
        P(("grp", "st"), None, None),
        P(("grp", "st"), None),
        P(),
        P(None, "tp"),
        P(None, "tp"),
        P(None, "tp"),
        P("tp"),
        P("tp", None),
        P(),
        P(),
        P(None, "tp"),
        P(None, "tp"),
        P(None, "tp"),
        P("tp", None),
        P(),
    )
    out_specs = P(("grp", "st", "tp"), None)
    return jax.shard_map(local, mesh=mesh, in_specs=in_specs, out_specs=out_specs, check_vma=False)
```

```python
import functools

import jax
import jax.numpy as jnp
from jax import lax
from jax.experimental import pallas as pl
from jax.experimental.pallas import tpu as pltpu
from jax.sharding import PartitionSpec as P

CA = 1024
HD = 256
SEQ_LEN = 128
CORES = 2
LANES = 128
EPS = 1e-06
EMPTY = -1e30
BACKLOG = {6: 9.0, 7: 0.8, 8: 0.15, 9: 0.15}
MESH = pl.DeviceIdType.MESH
F32 = jnp.float32
BF16 = jnp.bfloat16


def remote(src, dst, send_sem, recv_sem, **target):
    return pltpu.make_async_remote_copy(
        src_ref=src, dst_ref=dst, send_sem=send_sem, recv_sem=recv_sem,
        device_id=target, device_id_type=MESH,
    )


def place_of(distance, n):
    half = n // 2
    return jnp.where(distance >= half, 2 * (distance - half), 2 * (half - distance) - 1)


def order_of(n):
    half = n // 2
    order = [half]
    for j in range(1, half):
        order += [half - j, half + j]
    return order + [0]


def normed_rows(dst, src, gain, rows, step=16, unroll=2):
    @pl.loop(0, rows // step, unroll=unroll)
    def _(i):
        at = pl.ds(pl.multiple_of(i * step, step), step)
        x = src[at, :].astype(F32)
        inv = lax.rsqrt(jnp.mean(x * x, axis=-1, keepdims=True) + EPS)
        dst[at, :] = (x * inv * gain[...]).astype(BF16)


def merged(a, b):
    best = jnp.maximum(a[1], b[1])
    fa, fb = jnp.exp(a[1] - best), jnp.exp(b[1] - best)
    return fa * a[0] + fb * b[0], best, fa * a[2] + fb * b[2]


class Plan:
    def __init__(self):
        self.steps = {}

    def add(self, name, run, time, rank, after=(), gets=(), sends=()):
        self.steps[name] = (run, time, rank, tuple(after), tuple(gets), tuple(sends))

    def order(self, backlog):
        clock, free, arrival, done, order = 0.0, {}, {}, set(), []
        left = list(self.steps)
        while left:
            best = None
            for name in left:
                _, _, rank, after, gets, sends = self.steps[name]
                if all(a in done for a in after) and all(g in arrival for g in gets):
                    ready = max([clock] + [arrival[g] for g in gets])
                    if rank in backlog:
                        ready = max([ready] + [free.get(link, 0.0) - backlog[rank] for _, link, *_ in sends])
                    if best is None or (ready, rank) < best[0]:
                        best = ((ready, rank), name)
            (ready, _), name = best
            _, time, _, _, _, sends = self.steps[name]
            clock = ready + time
            for message, link, wire, late, *hops in sends:
                free[link] = max(free.get(link, 0.0), clock) + wire
                arrival[message] = free[link] + late
                free[link] += wire * (hops[0] - 1 if hops else 0)
            done.add(name)
            left.remove(name)
            order.append((name, ready, clock))
        return order


def step_plan(k):
    plan = Plan()
    ring, half, groups, xhalf = k.ring, k.half, k.groups, k.xhalf
    hop_late, far_late, q_wire, y_wire, x_wire = 2.4, 0.75, 1.4, 0.72, 1.4
    for g in range(groups):
        plan.add(
            ("q", g), functools.partial(k.queries, g), 0.76, 1, [("q", g - 1)] if g else [],
            sends=[(("q", side, 1, g), ("y", side), q_wire, hop_late) for side in range(2)],
        )
    for hop in range(1, half + 1):
        for g in range(groups):
            for side in range(2):
                if hop == half and (g < groups // 2) != (side == 0):
                    continue
                on = hop + 1 < half or (hop + 1 == half and (g < groups // 2) == (side == 0))
                plan.add(
                    ("hand", side, hop, g), functools.partial(k.hand_on, side, hop, g, on), 0.03, 0,
                    gets=[("q", side, hop, g)],
                    sends=[(("q", side, hop + 1, g), ("y", side), q_wire, hop_late)] if on else [],
                )
    pairs = list(range(0, k.passages, 2))
    for p in pairs:
        if p == 0:
            plan.add(("norm", p), functools.partial(k.norm_passages, p), 1.0, 20, [("q", groups - 1)])
        plan.add(("k", p), functools.partial(k.keys, p), 0.77, 20, [("v", p - 2) if p else ("norm", p)])
        plan.add(("v", p), functools.partial(k.values, p), 0.86, 20, [("k", p)], sends=[(("kv", p), ("core",), 0.4, 1.0)])
    plan.add(("here",), k.all_here, 0.65, 21, [("v", p) for p in pairs], gets=[("kv", p) for p in pairs])
    for rel in range(ring):
        hop = min(rel, ring - rel)
        if hop == half:
            hands = [("hand", 0 if g < groups // 2 else 1, hop, g) for g in range(groups)]
        elif hop:
            hands = [("hand", 1 if rel < half else 0, hop, g) for g in range(groups)]
        else:
            hands = []
        plan.add(("slots", rel), functools.partial(k.attend, rel), 0.6, 19 - hop, [("here",)] + hands)
        plan.add(("attend", rel), functools.partial(k.join, rel), 0.3, 1, [("slots", rel)])
    for rel in range(1, ring):
        hop = min(rel, ring - rel)
        plan.add(
            ("direct", rel), functools.partial(k.direct, rel), 0.04, 2, [("attend", rel)],
            sends=[(("direct", ring - rel), ("y", 0 if rel <= half else 1), y_wire, hop_late + far_late * (hop - 1), hop)],
        )
    for c, chunk in enumerate(k.chunks[1:], 1):
        for p in chunk:
            joined = k.join_side(p)
            if joined is not None:
                plan.add(
                    ("join", p), functools.partial(k.join_late, p), 0.04, 5 + c, [("attend", half)],
                    sends=[(("join", p), ("y", joined), y_wire, hop_late + far_late * (half - 2), half - 1)],
                )
            for side in range(2):
                far = k.start_of(side, p)
                for d in range(far, 0, -1):
                    rel = d if side == 0 else ring - d
                    gets = [] if d == far else [("y", side, p, d)]
                    if joined == side and d == 1:
                        gets = gets + [("join", p)]
                    plan.add(
                        ("y", side, p, d),
                        functools.partial(k.y_start if d == far else k.y_stage, side, p, d), 0.04 if d == far else 0.06,
                        5 + c, [("attend", rel)], gets=gets,
                        sends=[(("y", side, p, d - 1), ("y", side), y_wire, hop_late)],
                    )
    for g in range(groups):
        plan.add(("glu", g), functools.partial(k.glu, g), 0.95, 30, [("q", groups - 1)])
        plan.add(("conv", g), functools.partial(k.convolve, g), 0.25, 29, [("glu", g)])
    plan.add(("sums",), k.send_sums, 0.1, 3, [("conv", g) for g in range(groups)],
             sends=[(("sums",), ("x", 2), 0.5, 5.0)])
    plan.add(("act",), k.activations, 0.4, 4, gets=[("sums",)])
    for c, chunk in enumerate(k.chunks):
        if c == 0:
            gets = [("direct", rel) for rel in range(1, ring)]
        else:
            gets = [("y", side, p, 0) for p in chunk for side in range(2)]
        plan.add(("home", c), functools.partial(k.home, c), 0.3, 4, [("attend", 0)], gets=gets)
        dist = xhalf - c
        for t in range(k.tiles):
            h = t // (k.tiles // 2)
            if dist == xhalf:
                gets, outs = [], [h]
            elif dist == 0:
                gets, outs = [0, 1], []
            else:
                gets = [0, 1] if dist < xhalf - 1 else [h]
                outs = [0, 1]
            plan.add(
                ("project", c, t), functools.partial(k.project, c, t, gets, outs), 0.25, 3, [("home", c), ("act",)],
                gets=[("x", side, dist, t) for side in gets],
                sends=[(("x", side, dist - 1, t), ("x", side), x_wire, hop_late) for side in outs],
            )
    return plan


class Body:
    def __init__(self, n_st, n_tp, slots, blocks, per_block, refs):
        self.__dict__.update(refs)
        self.n_st, self.n_tp, self.slots, self.blocks, self.per_block = n_st, n_tp, slots, blocks, per_block
        self.ring, self.groups = n_st // CORES, self.tok_hbm.shape[0] // 128
        self.half, self.xhalf = self.ring // 2, n_tp // 2
        self.passages = self.store_hbm.shape[0]
        self.per_group = blocks // self.groups
        self.block_len = 128 // self.per_group
        self.width = self.tok_hbm.shape[1]
        self.tile = 512
        self.tiles = self.width // self.tile
        self.me, self.x_me = lax.axis_index("st"), lax.axis_index("tp")
        self.core, self.y_me = lax.rem(self.me, CORES), self.me // CORES
        self.partner = self.me + 1 - 2 * self.core
        self.right, self.left = self.chip(1), self.chip(self.ring - 1)
        self.waiting, self.unused, self.loads, self.clock = [], list(range(refs["send_sem"].shape[0])), [], 0.0
        self.early = 2
        self.places = order_of(n_tp)
        self.chunks = [[0]] + [[2 * j - 1, 2 * j] for j in range(1, self.xhalf)] + [[n_tp - 1]]
        self.start_cw = {}
        for c, chunk in enumerate(self.chunks):
            for i, p in enumerate(chunk):
                self.start_cw[p] = self.half if (i == 0 and c < len(self.chunks) - 1) else self.half - 1

    def chip(self, d):
        return lax.rem(self.me + CORES * d, self.n_st)

    def column(self, d):
        return lax.rem(self.x_me + d, self.n_tp)

    def send(self, src, dst, recv_sem, **target):
        self.send_all([(src, dst)], recv_sem, **target)

    def send_all(self, pairs, recv_sem, **target):
        if not self.unused:
            self.settle()
        at = self.unused.pop(0)
        sem = self.send_sem.at[at]
        for src, dst in pairs:
            remote(src, dst, sem, recv_sem, **target).start()
        whole = self.both if len(pairs) > 1 else pairs[0][0]
        self.waiting.append((self.clock, remote(whole, whole, sem, recv_sem, **target), at))

    def settle(self):
        _, copy, at = self.waiting.pop(0)
        copy.wait_send()
        self.unused.append(at)

    def got(self, ref, recv_sem):
        remote(ref, ref, self.send_sem.at[0], recv_sem, st=self.partner).wait_recv()

    def load(self, src, dst):
        copy = pltpu.make_async_copy(src, dst, self.load_sem.at[len(self.loads)])
        copy.start()
        self.loads.append(copy)
        return copy

    def start_of(self, side, p):
        if self.join_side(p) is not None:
            return self.half - 1
        return self.start_cw[p] if side == 0 else 2 * self.half - 1 - self.start_cw[p]

    def enter(self):
        barrier = pltpu.get_barrier_semaphore()
        for d in range(1, self.ring):
            pl.semaphore_signal(barrier, inc=1, device_id={"st": self.chip(d)}, device_id_type=MESH)
        pl.semaphore_signal(barrier, inc=1, device_id={"st": self.partner}, device_id_type=MESH)
        for d in range(1, self.n_tp):
            pl.semaphore_signal(barrier, inc=1, device_id={"tp": self.column(d)}, device_id_type=MESH)
        small = lambda name: self.load(getattr(self, name + "_hbm"), getattr(self, name))
        self.first_loads = [small("qgain"), self.load(self.wq_hbm, self.wq)]
        rows = lambda g: pl.ds(g * 128, 128)
        self.tok_loads = [self.load(self.tok_hbm.at[rows(g)], self.tok.at[rows(g)]) for g in range(self.groups)]
        self.ids_load = small("ids")
        self.kv_loads = [small("pgain"), self.load(self.wk_hbm, self.wk), self.load(self.wv_hbm, self.wv)]
        self.store_loads = [
            self.load(self.store_hbm.at[p], self.store.at[pl.ds(p * 128, 128)]) for p in range(self.passages)
        ]
        self.glu_loads = [
            small("mgain"), small("taps"), small("cgain"),
            self.load(self.gv_hbm, self.wglu.at[:, pl.ds(0, LANES)]),
            self.load(self.gg_hbm, self.wglu.at[:, pl.ds(LANES, LANES)]),
        ]
        self.out_loads = [small("blend"), self.load(self.attn_hbm, self.attn), self.load(self.mix_hbm, self.mix)]
        s = self.slots
        self.outs[s] = jnp.zeros(self.outs.shape[1:], BF16)
        self.ml[s, 0:1] = jnp.full((1, LANES), EMPTY, F32)
        self.ml[s, 1:2] = jnp.zeros((1, LANES), F32)
        self.padded[...] = jnp.zeros(self.padded.shape, F32)

    def make_table(self):
        self.ids_load.wait()
        chip = lax.broadcasted_iota(jnp.int32, (self.ring, LANES), 0)
        lane = lax.broadcasted_iota(jnp.int32, (self.ring, LANES), 1)
        used = jnp.zeros((self.ring, LANES), jnp.int32)
        table = jnp.zeros((self.ring, LANES), jnp.int32)
        held = CORES * self.passages
        for n in range(self.blocks * self.per_block):
            wanted = self.ids[n % self.per_block, n // self.per_block]
            owner = wanted // held
            here = (chip == owner) & (used < self.slots)
            table = jnp.where(here & (lane == used), n // self.per_block, table)
            table = jnp.where(here & (lane == self.slots + used), wanted - owner * held, table)
            table = jnp.where(lane == 2 * self.slots + n, jnp.where(here, used, self.slots), table)
            used = used + jnp.where(here, 1, 0)
        for i in range(self.ring):
            self.table[i] = table[i : i + 1]

    def entered(self):
        self.make_table()
        pl.semaphore_wait(pltpu.get_barrier_semaphore(), self.ring + self.n_tp - 1)
        for d in range(1, self.ring):
            self.send(self.table.at[lax.rem(self.y_me + d, self.ring)], self.tabv.at[self.ring - d], self.t_recv.at[0],
                      st=self.chip(d))
        self.own_table = pltpu.make_async_copy(self.table.at[self.y_me], self.tabv.at[0], self.s_sem.at[1])
        self.own_table.start()


    def part(self, rel, g):
        return self.qall[rel].at[pl.ds(self.per_group * g, self.per_group)]

    def queries(self, g):
        self.tok_loads[g].wait()
        if g == 0:
            self.first_loads[0].wait()
        normed_rows(self.xq, self.tok.at[pl.ds(g * 128, 128)], self.qgain, 128, unroll=4)
        if g == 0:
            self.first_loads[1].wait()
        q = jnp.dot(self.xq[...], self.wq[...], preferred_element_type=F32).astype(BF16)
        n = self.block_len
        for i in range(self.per_group):
            self.qall[0][self.per_group * g + i] = q[i * n : (i + 1) * n]
        if g == 0:
            with jax.named_scope("entry"):
                self.entered()
        for side, rel, who in ((0, self.ring - 1, self.right), (1, 1, self.left)):
            self.send(self.part(0, g), self.part(rel, g), self.q_recv.at[self.q_sem(side, 1, g)], st=who)

    def hand_on(self, side, hop, g, on):
        rel = self.ring - hop if side == 0 else hop
        here = self.part(rel, g)
        self.got(here, self.q_recv.at[self.q_sem(side, hop, g)])
        if on:
            there = self.part(rel - 1 if side == 0 else rel + 1, g)
            self.send(here, there, self.q_recv.at[self.q_sem(side, hop + 1, g)],
                      st=self.right if side == 0 else self.left)

    def q_sem(self, side, hop, g):
        last = (self.half - 1) * self.groups
        each = last + self.groups // 2
        return side * each + ((hop - 1) * self.groups + g if hop < self.half else last + g % (self.groups // 2))


    def norm_passages(self, p):
        for copy in self.kv_loads + self.store_loads[:2]:
            copy.wait()
        self.norm_half(p, 0, unroll=2)
        self.norm_half(p, 1, unroll=2)

    def norm_half(self, p, i, unroll=8):
        if p < self.passages:
            if p:
                self.store_loads[p + i].wait()
            normed_rows(self.xn.at[p // 2 % 2, pl.ds(i * 128, 128)], self.store.at[pl.ds((p + i) * 128, 128)], self.pgain,
                        128, unroll=unroll)

    def share(self, j, ref, p):
        both = ref.at[pl.ds(self.core * self.passages + p, 2)]
        self.send(both, both, self.kv_recv.at[j], st=self.partner)

    def keys(self, p):
        self.norm_half(p + 2, 0)
        k = jnp.dot(self.xn[p // 2 % 2], self.wk[...], preferred_element_type=F32).astype(BF16)
        for i in range(2):
            at = self.core * self.passages + p + i
            self.kall[at] = k[i * 128 : (i + 1) * 128]
        self.share(0, self.kall, p)

    def values(self, p):
        self.norm_half(p + 2, 1)
        v = jnp.dot(self.xn[p // 2 % 2], self.wv[...], preferred_element_type=F32)
        for i in range(2):
            at = self.core * self.passages + p + i
            w = v[i * 128 : (i + 1) * 128]
            self.vall[at] = jnp.concatenate([w[:, :LANES].T, w[:, LANES:].T], axis=1).astype(BF16)
        self.share(1, self.vall, p)

    def all_here(self):
        for j, ref in enumerate((self.kall, self.vall)):
            self.got(ref.at[pl.ds((1 - self.core) * self.passages, self.passages)], self.kv_recv.at[j])
        self.own_table.wait()
        self.got(self.tabv.at[pl.ds(1, self.ring - 1)], self.t_recv.at[0])
        to_scalar = pltpu.make_async_copy(self.tabv, self.tabs, self.s_sem.at[0])
        to_scalar.start()
        to_scalar.wait()


    def attend(self, rel):
        low_half = lax.broadcasted_iota(jnp.int32, (LANES, LANES), 1) < LANES // 2
        slots, tabs, ml, outs = self.slots, self.tabs, self.ml, self.outs
        for k in range(slots):
            q = self.qall[rel][tabs[rel, 0, k]]
            p = tabs[rel, 0, slots + k]
            s = lax.dot_general(
                self.kall[p], jnp.concatenate([q, q], axis=0), (((1,), (1,)), ((), ())), preferred_element_type=F32
            ) * HD ** (-0.5)
            top = jnp.max(s, axis=0, keepdims=True)
            e = jnp.exp(s - top)
            ml[k, 0:1] = top
            ml[k, 1:2] = jnp.sum(e, axis=0, keepdims=True)
            w = jnp.concatenate([jnp.where(low_half, e, 0.0), jnp.where(low_half, 0.0, e)], axis=0).astype(BF16)
            outs[k] = jnp.dot(self.vall[p], w, preferred_element_type=F32).astype(BF16)

    def join(self, rel):
        slots, tabs, ml, outs = self.slots, self.tabs, self.ml, self.outs

        @pl.loop(0, self.blocks, unroll=4)
        def _(distance):
            b = lax.rem(self.x_me + distance, self.blocks)
            at = [tabs[rel, 0, 2 * slots + b * self.per_block + j] for j in range(self.per_block)]
            mls = [ml[i] for i in at]
            best = functools.reduce(jnp.maximum, [a[0:1] for a in mls])
            scale = [jnp.exp(a[0:1] - best) for a in mls]
            total = sum(f * a[1:2] for f, a in zip(scale, mls))
            num = sum(f * outs[i].astype(F32) for f, i in zip(scale, at))
            place = place_of(distance, self.n_tp)
            self.acc[rel, place] = num.astype(BF16)
            self.stats[rel, place, 0:1] = best
            self.stats[rel, place, 1:2] = total


    def y_out(self, side, p, d, num, stat):
        who = self.right if side == 0 else self.left
        pairs = [(num, self.ydata.at[side, p, d - 1]), (stat, self.ystat.at[side, p, d - 1])]
        self.send_all(pairs, self.y_recv.at[self.y_sem(side, p, d - 1)], st=who)

    def y_sem(self, side, p, d):
        return sum(self.start_of(i, q) for q in range(1, p) for i in range(2)) + side * self.start_of(0, p) + d

    def y_start(self, side, p, d):
        rel = d if side == 0 else self.ring - d
        self.y_out(side, p, d, self.acc.at[rel, p], self.stats.at[rel, p])

    def y_arrived(self, side, p, d):
        self.got(self.both, self.y_recv.at[self.y_sem(side, p, d)])
        stat = self.ystat.at[side, p, d]
        return self.ydata[side, p, d].astype(F32), stat[0:1], stat[1:2]

    def own(self, rel, p):
        return self.acc[rel, p].astype(F32), self.stats[rel, p, 0:1], self.stats[rel, p, 1:2]

    def y_stage(self, side, p, d):
        so_far = merged(self.y_arrived(side, p, d), self.own(d if side == 0 else self.ring - d, p))
        if d == 1 and self.join_side(p) == side:
            so_far = merged(so_far, self.joined(p))
        num, best, total = so_far
        self.ydata[side, p, d] = num.astype(BF16)
        self.ystat[side, p, d, 0:1] = best
        self.ystat[side, p, d, 1:2] = total
        self.y_out(side, p, d, self.ydata.at[side, p, d], self.ystat.at[side, p, d])

    def join_side(self, p):
        early = [q for chunk in self.chunks[1 : self.early] for q in chunk]
        return early.index(p) % 2 if p in early else None

    def join_late(self, p):
        side = self.join_side(p)
        hops = self.half - 1
        who = self.chip(hops if side == 0 else self.ring - hops)
        pairs = [(self.acc.at[self.half, p], self.jdata.at[p]), (self.stats.at[self.half, p], self.jstat.at[p])]
        self.send_all(pairs, self.j_recv.at[p], st=who)

    def joined(self, p):
        self.got(self.both, self.j_recv.at[p])
        stat = self.jstat.at[p]
        return self.jdata[p].astype(F32), stat[0:1], stat[1:2]

    def direct(self, rel):
        p = self.chunks[0][0]
        at = self.ring - rel
        pairs = [(self.acc.at[rel, p], self.ddata.at[at]), (self.stats.at[rel, p], self.dstat.at[at])]
        self.send_all(pairs, self.d_recv.at[at - 1], st=self.chip(rel))

    def home(self, c):
        for i, p in enumerate(self.chunks[c]):
            if c == 0:
                so_far = self.own(0, p)
                for rel in range(1, self.ring):
                    self.got(self.both, self.d_recv.at[rel - 1])
                    stat = self.dstat.at[rel]
                    so_far = merged(so_far, (self.ddata[rel].astype(F32), stat[0:1], stat[1:2]))
            else:
                so_far = merged(merged(self.y_arrived(0, p, 0), self.own(0, p)), self.y_arrived(1, p, 0))
            num, best, total = so_far
            t = (num / total).T.astype(BF16)
            n = self.block_len
            self.rows_a[c, pl.ds(i * n, n), :] = jnp.concatenate([t[:n], t[n:]], axis=1)


    def glu(self, g):
        xm = self.xm
        if g == 0:
            for copy in self.glu_loads:
                copy.wait()
        normed_rows(xm, self.tok.at[pl.ds(g * 128, 128)], self.mgain, 128)
        y = jnp.dot(xm[...], self.wglu[...], preferred_element_type=F32)
        gated = y[:, :LANES] * jax.nn.sigmoid(y[:, LANES:])
        self.padded[g, pl.ds(16, 128), :] = gated.astype(BF16).astype(F32)

    def convolve(self, g):
        taps = self.taps[...].astype(F32)
        span = taps.shape[0]
        first = 16 - (span - 1) // 2
        running = jnp.zeros((128, LANES), F32)
        for k in range(span):
            running = running + self.padded[g, pl.ds(first + k, 128), :] * taps[k : k + 1]
        self.conv[g] = running
        turned = running.T
        self.sums[g : g + 1, :] = jnp.sum(turned, axis=0, keepdims=True)
        at = self.groups + g
        self.sums[at : at + 1, :] = jnp.sum(turned * turned, axis=0, keepdims=True)

    def send_sums(self):
        for d in range(1, self.n_tp):
            self.send(self.sums, self.allsums.at[self.n_tp - d], self.c_recv.at[0], tp=self.column(d))

    def activations(self):
        total = self.sums[...]
        self.got(self.allsums.at[pl.ds(1, self.n_tp - 1)], self.c_recv.at[0])
        for d in range(1, self.n_tp):
            total = total + self.allsums[d]
        groups = self.groups
        mean = total[:groups] / CA
        var = total[groups:] / CA - mean * mean
        cols = jnp.concatenate([mean, lax.rsqrt(var + EPS)], axis=0).T
        n = self.block_len
        for g in range(groups):
            z = (self.conv[g] - cols[:, g : g + 1]) * cols[:, groups + g : groups + g + 1] * self.cgain[...]
            z = (z / (1.0 + jnp.exp(-z))).astype(BF16)
            for i in range(self.per_group):
                self.act[g * self.per_group + i] = z[i * n : (i + 1) * n]


    def project(self, c, t, gets, outs):
        chunk, k, n = self.chunks[c], self.xhalf - c, self.block_len
        at = pl.ds(t * self.tile, self.tile)
        if c == 0 and t == 0:
            for copy in self.out_loads:
                copy.wait()
        rows_p = jnp.concatenate([self.act[self.column(self.places[p])] for p in chunk], axis=0)
        y = jnp.dot(rows_p, self.mix[:, at], preferred_element_type=F32) + self.blend[:, at] * jnp.dot(
            self.rows_a[c, pl.ds(0, n * len(chunk)), :], self.attn[:, at], preferred_element_type=F32
        )
        for side in gets:
            self.got(self.xdata.at[side, k, t], self.x_recv.at[self.x_sem(side, k, t)])
        if k == 0:
            y = y + self.xdata[0, k, t].astype(F32) + self.xdata[1, k, t].astype(F32)
            self.out[:, at] = y.astype(BF16)
            return
        for side in outs:
            mine = y if len(chunk) == 1 else y[side * n : (side + 1) * n]
            if side in gets:
                mine = mine + self.xdata[side, k, t].astype(F32)
            slot = self.xdata.at[side, k, t] if k < self.xhalf else self.xfirst.at[t]
            slot[...] = mine.astype(BF16)
            self.send(slot, self.xdata.at[side, k - 1, t], self.x_recv.at[self.x_sem(side, k - 1, t)],
                      tp=self.column(1 if side == 0 else self.n_tp - 1))

    def x_sem(self, side, k, t):
        return side * (self.xhalf - 1) * self.tiles + k * self.tiles + t if k < self.xhalf - 1 else (
            2 * (self.xhalf - 1) * self.tiles + t
        )


def whole_kernel(names, n_st, n_tp, slots, blocks, per_block, *refs):
    ring = n_st // CORES
    at = names.index("qall")
    found = dict(zip(names[:at] + names[at + 1 :], refs[:at] + refs[at + ring :]))
    found["qall"] = refs[at : at + ring]
    k = Body(n_st, n_tp, slots, blocks, per_block, found)
    plan = step_plan(k)
    with jax.named_scope("enter"):
        k.enter()
    for name, ready, end in plan.order(BACKLOG):
        gap = ready - k.clock
        while gap > 0.1 and k.waiting and k.waiting[0][0] < k.clock - 8.0:
            k.settle()
            gap -= 0.03
        with jax.named_scope("_".join(str(part) for part in name)):
            plan.steps[name][0]()
        k.clock = end
    with jax.named_scope(f"tail_{len(k.waiting)}"):
        while k.waiting:
            k.settle()


def whole(ids, slots, blocks, per_block, big, small):
    n_st, n_tp = lax.axis_size("st"), lax.axis_size("tp")
    ring, half, xhalf = n_st // CORES, n_st // CORES // 2, n_tp // 2
    rows, width = big["tok_hbm"].shape
    passages, prows, _ = big["store_hbm"].shape
    groups, block_len, mine = rows // 128, rows // blocks, rows // n_tp
    channels = big["gv_hbm"].shape[1]
    assert prows == 128 and big["wq_hbm"].shape[1] == HD and channels == LANES
    assert block_len * 2 == LANES and blocks == n_tp and passages % 2 == 0
    tiles = width // 512
    dma = pltpu.SemaphoreType.DMA
    scratch = {
        "tok": pltpu.VMEM((rows, width), BF16),
        "store": pltpu.VMEM((passages * prows, width), BF16),
        "wq": pltpu.VMEM((width, HD), BF16),
        "wk": pltpu.VMEM((width, HD), BF16),
        "wv": pltpu.VMEM((width, HD), BF16),
        "wglu": pltpu.VMEM((width, 2 * LANES), BF16),
        "attn": pltpu.VMEM((HD, width), BF16),
        "mix": pltpu.VMEM((channels, width), BF16),
        "xq": pltpu.VMEM((128, width), BF16),
        "xn": pltpu.VMEM((2, 256, width), BF16),
        "xm": pltpu.VMEM((128, width), BF16),
        "kall": pltpu.VMEM((CORES * passages, prows, HD), BF16),
        "vall": pltpu.VMEM((CORES * passages, LANES, 2 * prows), BF16),
        "outs": pltpu.VMEM((slots + 1, LANES, LANES), BF16),
        "ml": pltpu.VMEM((slots + 1, 2, LANES), F32),
        "tabv": pltpu.VMEM((ring, 1, LANES), jnp.int32),
        "tabs": pltpu.SMEM((ring, 1, LANES), jnp.int32),
        "acc": pltpu.VMEM((ring, blocks, LANES, LANES), BF16),
        "stats": pltpu.VMEM((ring, blocks, 2, LANES), F32),
        "ydata": pltpu.VMEM((2, blocks, half, LANES, LANES), BF16),
        "ystat": pltpu.VMEM((2, blocks, half, 2, LANES), F32),
        "ddata": pltpu.VMEM((ring, LANES, LANES), BF16),
        "dstat": pltpu.VMEM((ring, 2, LANES), F32),
        "both": pltpu.VMEM((1 + LANES * LANES * 2 // (2 * LANES * 4), 2, LANES), F32),
        "jdata": pltpu.VMEM((blocks, LANES, LANES), BF16),
        "jstat": pltpu.VMEM((blocks, 2, LANES), F32),
        "rows_a": pltpu.VMEM((xhalf + 1, 2 * block_len, HD), BF16),
        "padded": pltpu.VMEM((groups, 128 + 32, LANES), F32),
        "conv": pltpu.VMEM((groups, 128, LANES), F32),
        "sums": pltpu.VMEM((2 * groups, 128), F32),
        "allsums": pltpu.VMEM((n_tp, 2 * groups, 128), F32),
        "act": pltpu.VMEM((blocks, block_len, channels), BF16),
        "xdata": pltpu.VMEM((2, xhalf, tiles, mine, 512), BF16),
        "xfirst": pltpu.VMEM((tiles, mine, 512), BF16),
        "load_sem": dma((7 + groups + passages + len(small) + 1,)),
        "send_sem": dma((32,)),
        "q_recv": dma((2 * ((half - 1) * groups + groups // 2),)),
        "kv_recv": dma((2,)),
        "t_recv": dma((1,)),
        "s_sem": dma((2,)),
        "y_recv": dma(((blocks - 1) * (2 * half - 1),)),
        "d_recv": dma((ring - 1,)),
        "j_recv": dma((3,)),
        "x_recv": dma((2 * (xhalf - 1) * tiles + tiles,)),
        "c_recv": dma((1,)),
        "qall": None,
    }
    scratch = {**{n[:-4]: pltpu.VMEM(a.shape, a.dtype) for n, a in small.items()},
               "table": pltpu.VMEM((ring, 1, LANES), jnp.int32), "ids": pltpu.SMEM(ids.shape[::-1], jnp.int32), **scratch}
    names = list(big) + list(small) + ["ids_hbm", "out"] + list(scratch)
    shapes = [s for n, s in scratch.items() if n != "qall"]
    shapes += [pltpu.VMEM((blocks, block_len, HD), BF16) for _ in range(ring)]
    vmem = pl.BlockSpec(memory_space=pltpu.VMEM)
    return pl.pallas_call(
        functools.partial(whole_kernel, names, n_st, n_tp, slots, blocks, per_block),
        out_shape=jax.ShapeDtypeStruct((mine, width), BF16),
        in_specs=[pl.BlockSpec(memory_space=pltpu.HBM)] * (len(big) + len(small) + 1),
        out_specs=vmem,
        scratch_shapes=shapes,
        compiler_params=pltpu.CompilerParams(
            collective_id=0, has_side_effects=True, vmem_limit_bytes=66_000_000
        ),
        name="whole",
    )(*big.values(), *small.values(), ids.T)


def local(
    tokens, store, passage_ids, mix_gain, glu_value, glu_gate, conv_taps, channel_gain, mix_out,
    query_gain, passage_gain, query_proj, key_proj, value_proj, attn_out, blend_gain,
):
    owners = lax.axis_size("st")
    blocks, per_block = passage_ids.shape
    slots = CORES * (2 * blocks * per_block // owners)
    big = {
        "tok_hbm": tokens, "store_hbm": store, "wq_hbm": query_proj, "wk_hbm": key_proj, "wv_hbm": value_proj,
        "gv_hbm": glu_value, "gg_hbm": glu_gate, "attn_hbm": attn_out, "mix_hbm": mix_out,
    }
    small = {
        "qgain_hbm": query_gain[None], "pgain_hbm": passage_gain[None], "mgain_hbm": mix_gain[None], "taps_hbm": conv_taps,
        "cgain_hbm": channel_gain[None], "blend_hbm": blend_gain[None],
    }
    return whole(passage_ids, slots, blocks, per_block, big, small)


def solution(mesh):
    in_specs = (
        P(("grp", "st"), None),
        P(("grp", "st"), None, None),
        P(("grp", "st"), None),
        P(),
        P(None, "tp"),
        P(None, "tp"),
        P(None, "tp"),
        P("tp"),
        P("tp", None),
        P(),
        P(),
        P(None, "tp"),
        P(None, "tp"),
        P(None, "tp"),
        P("tp", None),
        P(),
    )
    out_specs = P(("grp", "st", "tp"), None)
    return jax.shard_map(local, mesh=mesh, in_specs=in_specs, out_specs=out_specs, check_vma=False)
```
